256 devices in a mesh: sp: 32 (over z, y), tp: 8 (over x, core).
Axes of the slice: x: 4, y: 4, z: 8, core: 2. Of those that a mesh axis runs over, the one named last changes fastest.
Arguments:
- frames: bfloat16 [8, 4096, 1024], P('tp', 'sp'), may hold values from -22 to 22
- norm_gain: float32 [1024], replicated, may hold values from 0.5 to 1.5
- conv_value_w: bfloat16 [1024, 512], P(None, 'tp'), may hold values from -0.1875 to 0.1875
- conv_gate_w: bfloat16 [1024, 512], P(None, 'tp'), may hold values from -0.1875 to 0.1875
- conv_taps: bfloat16 [31, 512], P(None, 'tp'), may hold values from -1 to 1
- conv_bias: float32 [512], P('tp'), may hold values from -1.2 to 1.2
- channel_gain: float32 [512], P('tp'), may hold values from 0.5 to 1.5
- channel_shift: float32 [512], P('tp'), may hold values from -1.2 to 1.2
- query_w: bfloat16 [1024, 1024], P(None, 'tp'), may hold values from -0.1875 to 0.1875
- forget_w: bfloat16 [1024, 1024], P(None, 'tp'), may hold values from -0.1875 to 0.1875
- input_w: bfloat16 [1024, 1024], P(None, 'tp'), may hold values from -0.1875 to 0.1875
- gate_w: bfloat16 [1024, 1024], P(None, 'tp'), may hold values from -0.1875 to 0.1875
- memory_rate: float32 [1024], P('tp'), may hold values from 0.5 to 32
- head_gain: float32 [1024], P('tp'), may hold values from 0.5 to 1.5
- conv_out_w: bfloat16 [512, 1024], P('tp'), may hold values from -0.1875 to 0.1875
- rec_out_w: bfloat16 [1024, 1024], P('tp'), may hold values from -0.125 to 0.125
Outputs:
- mixed: bfloat16 [8, 4096, 1024], P('tp', 'sp')
The draws below stay inside these ranges and needn't reach their ends.
All inputs are finite; a program needn't handle non-finite values.
Results may differ from the reference program's by a relative error of at most 0.015.
The reference program's roundings to bfloat16 on the way (of `normed`, `gated_conv`, `conv_out`, `scores`, `carried_low` and `rec_out`) count: a program that leaves them out, or rounds other values in their place, can miss the bound.
Values may be sent and summed in bfloat16 or wider, within the bound.
A program may use at most 64 MiB of HBM per device.

```python
import math
import jax
import jax.numpy as jnp
from jax import lax

D = 1024
D_CONV = 512
CONV_WIDTH = 31
HEADS = 8
HEAD = 128
D_HG = 1024
POS_DEV = 128
SEQS = 8
SEQ_LEN = 4096
N_SP = 32


def draw_frames(key, part):
    noise_key = jax.random.fold_in(key, 11)
    direction_key = jax.random.fold_in(key, 12)
    level_key = jax.random.fold_in(key, 13)
    block_count = SEQ_LEN // POS_DEV
    noise = jnp.clip(jax.random.normal(noise_key, (SEQS, SEQ_LEN, D), jnp.float32), -6.0, 6.0)
    direction = jnp.clip(jax.random.normal(direction_key, (D,), jnp.float32), -4.0, 4.0)
    levels = jax.random.uniform(level_key, (SEQS, block_count, 1, 1), jnp.float32, -4.0, 4.0)
    spread_levels = jnp.broadcast_to(levels, (SEQS, block_count, POS_DEV, 1)).reshape(SEQS, SEQ_LEN, 1)
    return (noise + spread_levels * direction).astype(jnp.bfloat16)


def shard_levels(stream_key, extent, pieces, low, largest):
    def one(dim, blocks):
        draws = jax.random.uniform(jax.random.fold_in(jax.random.fold_in(stream_key, 6), dim), (blocks,), jnp.float32, low / len(pieces), largest / len(pieces))
        return jnp.repeat(jnp.exp(draws), extent[dim] // blocks).reshape((-1,) + (1,) * (len(extent) - dim - 1))

    gain = one(*pieces[0])
    for cut in pieces[1:]:
        gain = gain * one(*cut)
    return gain


def bell_draw(key, dims, deviation, most, shards=(), held_as=jnp.bfloat16):
    values = deviation * jax.random.normal(key, dims, jnp.float32)
    if shards:
        values = values * shard_levels(key, dims, shards, -0.22, 0.18)
    return jnp.clip(values, -most, most).astype(held_as)


def setup_inputs(seed: int = 0) -> dict:
    arg_keys = jax.random.split(jax.random.key(seed), 17)
    return {
        "frames": draw_frames(jax.random.fold_in(arg_keys[16], 71), 0),
        "norm_gain": jnp.clip(1.0 + 0.1 * jax.random.normal(arg_keys[1], (D,), jnp.float32), 0.5, 1.5),
        "conv_value_w": bell_draw(arg_keys[2], (D, D_CONV), D ** -0.5, 0.1875, ((1, 8),)),
        "conv_gate_w": bell_draw(arg_keys[3], (D, D_CONV), D ** -0.5, 0.1875, ((1, 8),)),
        "conv_taps": bell_draw(arg_keys[4], (CONV_WIDTH, D_CONV), CONV_WIDTH ** -0.5, 1.0, ((1, 8),)),
        "conv_bias": bell_draw(arg_keys[5], (D_CONV,), 0.2, 1.2, ((0, 8),), jnp.float32),
        "channel_gain": jnp.clip(1.0 + 0.1 * jax.random.normal(arg_keys[6], (D_CONV,), jnp.float32), 0.5, 1.5),
        "channel_shift": bell_draw(arg_keys[7], (D_CONV,), 0.2, 1.2, ((0, 8),), jnp.float32),
        "query_w": bell_draw(arg_keys[8], (D, D_HG), D ** -0.5, 0.1875, ((1, 8),)),
        "forget_w": bell_draw(arg_keys[9], (D, D_HG), D ** -0.5, 0.1875, ((1, 8),)),
        "input_w": bell_draw(arg_keys[10], (D, D_HG), D ** -0.5, 0.1875, ((1, 8),)),
        "gate_w": bell_draw(arg_keys[11], (D, D_HG), D ** -0.5, 0.1875, ((1, 8),)),
        "memory_rate": jnp.clip(jnp.exp(math.log(32.0) - 4.158883 * jax.random.uniform(arg_keys[12], (D_HG,), jnp.float32) ** shard_levels(arg_keys[12], (D_HG,), ((0, 8),), -0.2, 0.2)), 0.5, 32.0),
        "head_gain": jnp.clip(1.0 + 0.1 * jax.random.normal(arg_keys[13], (D_HG,), jnp.float32), 0.5, 1.5),
        "conv_out_w": bell_draw(arg_keys[14], (D_CONV, D), (2 * D_CONV) ** -0.5, 0.1875, ((0, 8),)),
        "rec_out_w": bell_draw(arg_keys[15], (D_HG, D), (2 * D_HG) ** -0.5, 0.125, ((0, 8),)),
    }


EPS = 1e-06

def reference(frames, norm_gain, conv_value_w, conv_gate_w, conv_taps, conv_bias, channel_gain, channel_shift, query_w, forget_w, input_w, gate_w, memory_rate, head_gain, conv_out_w, rec_out_w):
    values = frames.astype(jnp.float32)
    normed = (values * lax.rsqrt(lax.optimization_barrier(jnp.mean(values * values, axis=-1, keepdims=True)) + EPS) * norm_gain).astype(jnp.bfloat16)
    flat_rows = normed.reshape(SEQS * SEQ_LEN, D)

    def project(weight):
        product = jnp.dot(flat_rows, weight, preferred_element_type=jnp.float32)
        return product.astype(jnp.bfloat16).reshape(SEQS, SEQ_LEN, weight.shape[1])
    conv_value = project(conv_value_w)
    conv_gate = project(conv_gate_w)
    queries = project(query_w)
    forget_raw = project(forget_w)
    inputs = project(input_w)
    out_gate = project(gate_w)
    gated_conv = (conv_value.astype(jnp.float32) * jax.nn.sigmoid(conv_gate.astype(jnp.float32))).astype(jnp.bfloat16)
    filtered = lax.conv_general_dilated(gated_conv, conv_taps[:, None, :], window_strides=(1,), padding=[(CONV_WIDTH - 1, 0)], dimension_numbers=('NWC', 'WIO', 'NWC'), feature_group_count=D_CONV, preferred_element_type=jnp.float32) + conv_bias
    row_mean = lax.optimization_barrier(jnp.mean(filtered, axis=-1, keepdims=True))
    row_var = lax.optimization_barrier(jnp.mean(filtered * filtered, axis=-1, keepdims=True)) - row_mean * row_mean
    scaled = (filtered - row_mean) * lax.rsqrt(row_var + EPS) * channel_gain + channel_shift
    conv_out = jax.nn.silu(scaled).astype(jnp.bfloat16)
    head_shape = (SEQS, SEQ_LEN, HEADS, HEAD)
    rate_rows = (memory_rate / SEQ_LEN).reshape(HEADS, HEAD)
    in_gate = rate_rows * jax.nn.sigmoid(-forget_raw.astype(jnp.float32)).reshape(head_shape)
    log_forget = jnp.log1p(-in_gate)
    query_rows = queries.astype(jnp.float32).reshape(head_shape)
    value_rows = inputs.reshape(head_shape).astype(jnp.float32)

    def to_blocks(array):
        return array.reshape(SEQS, N_SP, POS_DEV, HEADS, HEAD).transpose(1, 0, 2, 3, 4)
    causal = jnp.tril(jnp.ones((POS_DEV, POS_DEV), dtype=bool))
    highest = lax.Precision.HIGHEST

    def advance(carry_state, block_inputs):
        block_query, block_gate, block_forget, block_value = block_inputs
        cumulative = jnp.cumsum(block_forget, axis=1)
        final_sum = cumulative[:, -1]
        grown = (block_query * jnp.exp(cumulative)).astype(jnp.bfloat16).astype(jnp.float32)
        shrunk = (block_gate * jnp.exp(-cumulative)).astype(jnp.bfloat16).astype(jnp.float32)
        weighted = (block_gate * jnp.exp(final_sum[:, None] - cumulative)).astype(jnp.bfloat16).astype(jnp.float32)
        scores = jnp.einsum('sthk,suhk->shtu', grown, shrunk, precision=highest)
        scores = jnp.where(causal, scores, 0.0).astype(jnp.bfloat16).astype(jnp.float32)
        carried_low = carry_state.astype(jnp.bfloat16).astype(jnp.float32)
        block_out = jnp.einsum('shtu,suhv->sthv', scores, block_value, precision=highest)
        block_out = block_out + jnp.einsum('sthk,shkv->sthv', grown, carried_low, precision=highest)
        new_state = jnp.exp(final_sum)[..., None] * carry_state + jnp.einsum('suhk,suhv->shkv', weighted, block_value, precision=highest)
        return (new_state, block_out)
    start_state = jnp.zeros((SEQS, HEADS, HEAD, HEAD), jnp.float32)
    blocks = (to_blocks(query_rows), to_blocks(in_gate), to_blocks(log_forget), to_blocks(value_rows))
    final_state, block_outs = lax.scan(advance, start_state, blocks)
    rec_raw = block_outs.transpose(1, 0, 2, 3, 4).reshape(head_shape)
    rec_norm = rec_raw * lax.rsqrt(lax.optimization_barrier(jnp.mean(rec_raw * rec_raw, axis=-1, keepdims=True)) + EPS) * head_gain.reshape(HEADS, HEAD)
    rec_out = (rec_norm.reshape(SEQS, SEQ_LEN, D_HG) * jax.nn.silu(out_gate.astype(jnp.float32))).astype(jnp.bfloat16)
    conv_part = jnp.dot(conv_out.reshape(SEQS * SEQ_LEN, D_CONV), conv_out_w, preferred_element_type=jnp.float32)
    rec_part = jnp.dot(rec_out.reshape(SEQS * SEQ_LEN, D_HG), rec_out_w, preferred_element_type=jnp.float32)
    return (conv_part + rec_part).astype(jnp.bfloat16).reshape(SEQS, SEQ_LEN, D)
```

```python
import jax
import jax.numpy as jnp
from jax import lax
from jax.experimental import pallas as pl
from jax.experimental.pallas import tpu as pltpu
from jax.sharding import Mesh
from jax.sharding import PartitionSpec as P

F32, BF16 = jnp.float32, jnp.bfloat16
MESH = pl.DeviceIdType.MESH
NZ, NY, NX = 8, 4, 4
EPS = 1e-06
POS, D, HEAD = 128, 1024, 128
TAPS, HALO = 31, 32
D_CONV = 512
SEQ_LEN = 4096
OFF = (0, -1, 1, 2)
SLOT_OF = {0: 0, 3: 1, 1: 2, 2: 3}
FG, IN, QU, GA, CV, CG = 0, 256, 512, 768, 1024, 1152
NT = (((1,), (1,)), ((), ()))
TN = (((0,), (0,)), ((), ()))


def dot(a, b):
    return jnp.dot(a, b, preferred_element_type=F32)


def remote(src, dst, send, recv, dev):
    return pltpu.make_async_remote_copy(
        src_ref=src, dst_ref=dst, send_sem=send, recv_sem=recv, device_id=dev, device_id_type=MESH
    )


def sigmoid(v):
    return 1.0 / (1.0 + jnp.exp(-v))


def kernel(
    frames, norm_gain, cvw, cgw, taps, cbias, cgain, cshift, qw, fw, iw, gw, rate, hgain, cow, row,
    out,
    fr_v, ng_v, taps_v, vec_v, hv_v, pk, xs, w, cvs, wc, wr,
    grown_b, inp_b, shr_b, gate_b, local_b,
    st_s, st_r, dec_s, dec_r, t_s, t_r, dd_s, dd_r, c_s, c_r,
    halo_s, halo_r, ext, filt, stat_s, stat_r, ac_s, ac_r, ar_s, ar_r, out_v,
    lsem, psend, precv, gsend, grecv, r1s, r1r, r2s, r2r, r3s, r3r, hs, hr, ss, sr,
    acs, acr, ars, arr, wxs, wxr, wfs, wfr,
):
    z, y, x, c = (lax.axis_index(a) for a in ("z", "y", "x", "c"))
    partner = {"c": 1 - c}

    def at_x(k):
        return {"x": lax.rem(x + k + NX, NX)}

    def at_y(k):
        return {"y": lax.rem(y + k, NY)}

    bar = pltpu.get_barrier_semaphore()

    def greet(dev):
        pl.semaphore_signal(bar, inc=1, device_id=dev, device_id_type=MESH)

    greet(partner)
    for k in (1, 2, 3):
        greet(at_x(k))
        greet(at_y(k))

    @pl.loop(0, z)
    def _(i):
        greet({"z": i})

    @pl.when((y == 0) & (z > 0))
    def _():
        greet({"z": z - 1, "y": NY - 1})

    loads = []

    def load(src, dst):
        copy = pltpu.make_async_copy(src, dst, lsem.at[len(loads)])
        copy.start()
        loads.append(copy)

    load(frames.at[0], fr_v)
    load(norm_gain, ng_v)
    load(taps, taps_v)
    load(cbias, vec_v.at[0])
    load(cgain, vec_v.at[1])
    load(cshift, vec_v.at[2])
    load(rate, hv_v.at[0])
    load(hgain, hv_v.at[1])
    n_small = len(loads)
    for k, ref in enumerate((fw, iw, qw, gw)):
        load(ref, w.at[:, pl.ds(256 * k, 128)])
    load(cvw, cvs.at[0, 0])
    load(cgw, cvs.at[0, 1])
    load(cow, wc.at[0, pl.ds(0, 64)])
    load(row, wr.at[0, pl.ds(0, 128)])
    for copy in loads[:n_small]:
        copy.wait()

    values = fr_v[...].astype(F32)
    scale = lax.rsqrt(jnp.mean(values * values, axis=-1, keepdims=True) + EPS)
    xs[0] = (values * scale * ng_v[...]).astype(BF16)
    pk[0] = jnp.zeros((40, 128), F32)
    pk[0, 0:TAPS, 0:64] = taps_v[...].astype(F32)
    for k in range(3):
        pk[0, 32 + k : 33 + k, 0:64] = vec_v[k]
    for k in range(2):
        pk[0, 35 + k : 36 + k, :] = hv_v[k]

    pl.semaphore_wait(bar, 7 + (NZ - 1 - z) + jnp.where((y == NY - 1) & (z < NZ - 1), 1, 0))

    def half(ref, s, h):
        return ref.at[s, pl.ds(64 * h, 64)]

    g = [
        remote(half(xs, 0, 0), half(xs, 1, 0), gsend.at[0], grecv.at[0], at_x(1)),
        remote(half(xs, 0, 1), half(xs, 2, 1), gsend.at[1], grecv.at[1], at_x(-1)),
        remote(half(xs, 0, 1), half(xs, 1, 1), gsend.at[2], grecv.at[2], at_x(1)),
        remote(half(xs, 0, 0), half(xs, 2, 0), gsend.at[3], grecv.at[3], at_x(-1)),
        remote(half(xs, 1, 0), half(xs, 3, 0), gsend.at[4], grecv.at[4], at_x(1)),
        remote(half(xs, 2, 1), half(xs, 3, 1), gsend.at[5], grecv.at[5], at_x(-1)),
    ]
    for copy in g[:4]:
        copy.start()

    p = []

    def pair(src, dst):
        copy = remote(src, dst, psend.at[len(p)], precv.at[len(p)], partner)
        copy.start()
        p.append(copy)

    for k, ref in enumerate((fw, iw)):
        pair(ref, w.at[:, pl.ds(256 * k + 128, 128)])
    pair(pk.at[0], pk.at[1])
    for k, ref in enumerate((qw, gw)):
        pair(ref, w.at[:, pl.ds(256 * k + 640, 128)])
    pair(cvw, cvs.at[1, 0])
    pair(cgw, cvs.at[1, 1])
    pair(cow, wc.at[0, pl.ds(64, 64)])
    pair(row, wr.at[0, pl.ds(128, 128)])

    for copy in loads[n_small:]:
        copy.wait()
    for copy in p[:7]:
        copy.wait_recv()

    w[:, CV : CV + 128] = jnp.concatenate([cvs[0, 0], cvs[1, 0]], axis=1)
    w[:, CG : CG + 128] = jnp.concatenate([cvs[0, 1], cvs[1, 1]], axis=1)

    def conv_rows(a, b):
        return jnp.concatenate([pk[0, a:b, 0:64], pk[1, a:b, 0:64]], axis=1)

    tap_rows = conv_rows(0, 32)
    bias_row, gain_row, shift_row = (conv_rows(32 + k, 33 + k) for k in range(3))
    rate_row = jnp.concatenate([pk[0, 35:36], pk[1, 35:36]], axis=1) / SEQ_LEN
    hgain_row = jnp.concatenate([pk[0, 36:37], pk[1, 36:37]], axis=1)

    at_t = lax.broadcasted_iota(jnp.int32, (POS, POS), 0)
    at_u = lax.broadcasted_iota(jnp.int32, (POS, POS), 1)
    causal = at_u <= at_t
    tril = jnp.where(causal, 1.0, 0.0).astype(BF16)

    started = []

    def begin(j):
        rows = xs[j]
        forget_raw = dot(rows, w[:, FG : FG + 256]).astype(BF16).astype(F32)
        inputs = dot(rows, w[:, IN : IN + 256]).astype(BF16)
        in_gate = rate_row * sigmoid(-forget_raw)
        log_forget = jnp.log1p(-in_gate)
        hi = log_forget.astype(BF16)
        rest = log_forget - hi.astype(F32)
        mid = rest.astype(BF16)
        low = (rest - mid.astype(F32)).astype(BF16)
        cumulative = dot(tril, hi) + dot(tril, mid) + dot(tril, low)
        last = cumulative[POS - 1 : POS]
        weighted = (in_gate * jnp.exp(last - cumulative)).astype(BF16)
        for h in range(2):
            lanes = slice(128 * h, 128 * h + 128)
            state = lax.dot_general(
                inputs[:, lanes], weighted[:, lanes], TN, preferred_element_type=F32
            )
            for k in range(NY):
                st_s[j, k, 32 * h : 32 * h + 32] = state[32 * k : 32 * k + 32]
            dec_s[j, h : h + 1] = jnp.exp(last[:, lanes])
        st_r[j, y] = st_s[j, y]
        dec_r[j, y] = dec_s[j]
        for k in (1, 2, 3):
            to = lax.rem(y + k, NY)
            a = remote(st_s.at[j, to], st_r.at[j, y], r1s.at[j, k, 0], r1r.at[j, k, 0], {"y": to})
            b = remote(dec_s.at[j], dec_r.at[j, y], r1s.at[j, k, 1], r1r.at[j, k, 1], {"y": to})
            a.start()
            b.start()
            started.extend((a, b))
        conv_value = dot(rows, w[:, CV : CV + 128]).astype(BF16).astype(F32)
        conv_gate = dot(rows, w[:, CG : CG + 128]).astype(BF16).astype(F32)
        gated = (conv_value * sigmoid(conv_gate)).astype(BF16)
        halo_s[j] = gated[POS - HALO :]
        ext[j, HALO:] = gated.astype(F32)

        @pl.when(y < NY - 1)
        def _():
            remote(halo_s.at[j], halo_r.at[j], hs.at[j], hr.at[j], {"y": y + 1}).start()

        @pl.when((y == NY - 1) & (z < NZ - 1))
        def _():
            remote(halo_s.at[j], halo_r.at[j], hs.at[j], hr.at[j], {"z": z + 1, "y": 0}).start()

        queries = dot(rows, w[:, QU : QU + 256]).astype(BF16).astype(F32)
        grown = (queries * jnp.exp(cumulative)).astype(BF16)
        shrunk = (in_gate * jnp.exp(-cumulative)).astype(BF16)
        grown_b[j] = grown
        for h in range(2):
            lanes = slice(128 * h, 128 * h + 128)
            scores = lax.dot_general(
                grown[:, lanes], shrunk[:, lanes], NT, preferred_element_type=F32
            )
            scores = jnp.where(causal, scores, 0.0).astype(BF16)
            local_b[j, :, lanes] = dot(scores, inputs[:, lanes])
        gate_b[j] = dot(rows, w[:, GA : GA + 256]).astype(BF16)

    def spread(rows2):
        return jnp.concatenate(
            [jnp.broadcast_to(rows2[h : h + 1], (32, 128)) for h in range(2)], axis=0
        )

    def totals(j):
        for k in (1, 2, 3):
            remote(st_s.at[j, 0], st_r.at[j, 0], r1s.at[j, k, 0], r1r.at[j, k, 0], at_y(k)).wait_recv()
            remote(dec_s.at[j], dec_r.at[j, 0], r1s.at[j, k, 1], r1r.at[j, k, 1], at_y(k)).wait_recv()
        total = st_r[j, 0].astype(F32)
        decay = dec_r[j, 0]
        for k in (1, 2, 3):
            total = total * spread(dec_r[j, k]) + st_r[j, k].astype(F32)
            decay = decay * dec_r[j, k]
        t_s[j] = total
        dd_s[j] = decay

        @pl.loop(z + 1, NZ)
        def _(i):
            remote(t_s.at[j], t_r.at[j, z], r2s.at[j, i, 0], r2r.at[j, z, 0], {"z": i}).start()
            remote(dd_s.at[j], dd_r.at[j, z], r2s.at[j, i, 1], r2r.at[j, z, 1], {"z": i}).start()

    def carry(j):
        def step(i, state):
            remote(t_s.at[j], t_r.at[j, i], r2s.at[j, i, 0], r2r.at[j, i, 0], {"z": i}).wait_recv()
            remote(dd_s.at[j], dd_r.at[j, i], r2s.at[j, i, 1], r2r.at[j, i, 1], {"z": i}).wait_recv()
            return state * spread(dd_r[j, i]) + t_r[j, i].astype(F32)

        state = lax.fori_loop(0, z, step, jnp.zeros((64, 128), F32))
        for k in range(NY):
            c_s[j, k] = state.astype(BF16)
            if k < NY - 1:
                state = state * spread(dec_r[j, k]) + st_r[j, k].astype(F32)
        c_r[j, y] = c_s[j, y]
        for k in (1, 2, 3):
            to = lax.rem(y + k, NY)
            a = remote(c_s.at[j, to], c_r.at[j, y], r3s.at[j, k], r3r.at[j, k], {"y": to})
            a.start()
            started.append(a)

    def filtering(j):
        @pl.when((z > 0) | (y > 0))
        def _():
            remote(halo_s.at[j], halo_r.at[j], hs.at[j], hr.at[j], {"y": y}).wait_recv()
            ext[j, 0:HALO] = halo_r[j].astype(F32)

        @pl.when((z == 0) & (y == 0))
        def _():
            ext[j, 0:HALO] = jnp.zeros((HALO, 128), F32)

        acc = jnp.broadcast_to(bias_row, (POS, 128))
        for k in range(TAPS):
            first = HALO - (TAPS - 1) + k
            acc = acc + tap_rows[k : k + 1] * ext[j, first : first + POS]
        filt[j] = acc
        return jnp.sum(acc, axis=-1, keepdims=True), jnp.sum(acc * acc, axis=-1, keepdims=True)

    def conv_norm(j, sums, squares):
        mean = sums / D_CONV
        var = squares / D_CONV - mean * mean
        scaled = (filt[j] - mean) * lax.rsqrt(var + EPS) * gain_row + shift_row
        return (scaled * sigmoid(scaled)).astype(BF16)

    def finish(j):
        for k in (1, 2, 3):
            remote(c_s.at[j, 0], c_r.at[j, 0], r3s.at[j, k], r3r.at[j, k], at_y(k)).wait_recv()
        gate = gate_b[j].astype(F32)
        silu = gate * sigmoid(gate)
        parts = []
        for h in range(2):
            lanes = slice(128 * h, 128 * h + 128)
            low = jnp.concatenate([c_r[j, k, 32 * h : 32 * h + 32] for k in range(NY)], axis=0)
            raw = local_b[j, :, lanes] + lax.dot_general(
                grown_b[j, :, lanes], low, NT, preferred_element_type=F32
            )
            scale = lax.rsqrt(jnp.mean(raw * raw, axis=-1, keepdims=True) + EPS)
            parts.append((raw * scale * hgain_row[:, lanes] * silu[:, lanes]).astype(BF16))
        return jnp.concatenate(parts, axis=1)

    begin(0)
    g[0].wait_recv()
    g[4].start()
    g[1].wait_recv()
    g[5].start()
    wx = []
    for n, k in enumerate((1, -1, 2)):
        s = SLOT_OF[-k % NX]
        a = remote(cow, wc.at[s, pl.ds(0, 64)], wxs.at[0, n], wxr.at[0, n], at_x(k))
        b = remote(row, wr.at[s, pl.ds(0, 128)], wxs.at[1, n], wxr.at[1, n], at_x(k))
        a.start()
        b.start()
        wx.append((s, a, b))
    g[2].wait_recv()
    begin(1)
    totals(0)
    g[3].wait_recv()
    begin(2)
    totals(1)
    carry(0)
    g[4].wait_recv()
    g[5].wait_recv()
    begin(3)
    totals(2)
    carry(1)
    sums = [filtering(j) for j in range(3)]
    totals(3)
    sums.append(filtering(3))
    lane = lax.broadcasted_iota(jnp.int32, (POS, 128), 1)
    packed = jnp.zeros((POS, 128), F32)
    for j in range(4):
        packed = jnp.where(lane == j, sums[j][0], packed)
        packed = jnp.where(lane == 4 + j, sums[j][1], packed)
    stat_s[...] = packed.T[0:8]
    stats = []
    for n, k in enumerate((1, -1, 2)):
        s = SLOT_OF[-k % NX]
        a = remote(stat_s, stat_r.at[s], ss.at[n], sr.at[n], at_x(k))
        a.start()
        stats.append(a)
    carry(2)
    for a in stats:
        a.wait_recv()
    total = stat_s[...]
    sub = lax.broadcasted_iota(jnp.int32, (8, 128), 0)
    for s in (1, 2, 3):
        got = stat_r[s]
        order = [SLOT_OF[(OFF[j] - OFF[s]) % NX] for j in range(4)]
        total = total + jnp.concatenate(
            [got[base + k : base + k + 1] for base in (0, 4) for k in order], axis=0
        )
    columns = jnp.concatenate([total, jnp.zeros((120, 128), F32)], axis=0).T
    actc = []
    for j in range(4):
        rows = conv_norm(j, columns[:, j : j + 1], columns[:, 4 + j : 5 + j])
        if j == 0:
            ac_r[0] = rows
        else:
            ac_s[j] = rows
            a = remote(ac_s.at[j], ac_r.at[SLOT_OF[-OFF[j] % NX]], acs.at[j], acr.at[SLOT_OF[-OFF[j] % NX]], at_x(OFF[j]))
            a.start()
            actc.append(a)
    carry(3)
    wf = []
    for n, (s, a, b) in enumerate(wx):
        a.wait_recv()
        b.wait_recv()
        for m, (ref, size) in enumerate(((wc, 64), (wr, 128))):
            f = remote(ref.at[s, pl.ds(0, size)], ref.at[s, pl.ds(size, size)], wfs.at[m, n], wfr.at[m, n], partner)
            f.start()
            wf.append(f)
    actr = []
    for j in (1, 2, 3, 0):
        rows = finish(j)
        if j == 0:
            ar_r[0] = rows
        else:
            ar_s[j] = rows
            a = remote(ar_s.at[j], ar_r.at[SLOT_OF[-OFF[j] % NX]], ars.at[j], arr.at[SLOT_OF[-OFF[j] % NX]], at_x(OFF[j]))
            a.start()
            actr.append(a)
    for copy in p[7:]:
        copy.wait_recv()
    for f in wf:
        f.wait_recv()
    acc = dot(ac_r[0], wc[0]) + dot(ar_r[0], wr[0])
    for j in (1, 2, 3):
        remote(ac_s.at[j], ac_r.at[j], acs.at[j], acr.at[j], partner).wait_recv()
        acc = acc + dot(ac_r[j], wc[j])
    for j in (1, 2, 3):
        remote(ar_s.at[j], ar_r.at[j], ars.at[j], arr.at[j], partner).wait_recv()
        acc = acc + dot(ar_r[j], wr[j])
    out_v[...] = acc.astype(BF16)
    done = pltpu.make_async_copy(out_v, out.at[0], lsem.at[0])
    done.start()
    for a in g + p + started + stats + actc + actr + wf + [c for t in wx for c in t[1:]]:
        a.wait_send()

    for j in range(4):
        @pl.loop(z + 1, NZ)
        def _(i):
            remote(t_s.at[j], t_r.at[j, z], r2s.at[j, i, 0], r2r.at[j, z, 0], {"z": i}).wait_send()
            remote(dd_s.at[j], dd_r.at[j, z], r2s.at[j, i, 1], r2r.at[j, z, 1], {"z": i}).wait_send()

        @pl.when((y < NY - 1) | (z < NZ - 1))
        def _():
            remote(halo_s.at[j], halo_r.at[j], hs.at[j], hr.at[j], {"y": y}).wait_send()

    done.wait()


def local(
    frames, norm_gain, conv_value_w, conv_gate_w, conv_taps, conv_bias, channel_gain, channel_shift,
    query_w, forget_w, input_w, gate_w, memory_rate, head_gain, conv_out_w, rec_out_w,
):
    dma = pltpu.SemaphoreType.DMA
    scratch = [
        pltpu.VMEM((POS, D), BF16),
        pltpu.VMEM((1, D), F32),
        pltpu.VMEM((TAPS, 64), BF16),
        pltpu.VMEM((3, 1, 64), F32),
        pltpu.VMEM((2, 1, 128), F32),
        pltpu.VMEM((2, 40, 128), F32),
        pltpu.VMEM((4, POS, D), BF16),
        pltpu.VMEM((D, 1280), BF16),
        pltpu.VMEM((2, 2, D, 64), BF16),
        pltpu.VMEM((4, 128, D), BF16),
        pltpu.VMEM((4, 256, D), BF16),
        pltpu.VMEM((4, POS, 256), BF16),
        pltpu.VMEM((4, POS, 256), BF16),
        pltpu.VMEM((4, POS, 256), BF16),
        pltpu.VMEM((4, POS, 256), BF16),
        pltpu.VMEM((4, POS, 256), F32),
        pltpu.VMEM((4, NY, 64, 128), F32),
        pltpu.VMEM((4, NY, 64, 128), F32),
        pltpu.VMEM((4, 2, 128), F32),
        pltpu.VMEM((4, NY, 2, 128), F32),
        pltpu.VMEM((4, 64, 128), F32),
        pltpu.VMEM((4, NZ, 64, 128), F32),
        pltpu.VMEM((4, 2, 128), F32),
        pltpu.VMEM((4, NZ, 2, 128), F32),
        pltpu.VMEM((4, NY, 64, 128), BF16),
        pltpu.VMEM((4, NY, 64, 128), BF16),
        pltpu.VMEM((4, HALO, 128), BF16),
        pltpu.VMEM((4, HALO, 128), BF16),
        pltpu.VMEM((4, HALO + POS, 128), F32),
        pltpu.VMEM((4, POS, 128), F32),
        pltpu.VMEM((8, 128), F32),
        pltpu.VMEM((4, 8, 128), F32),
        pltpu.VMEM((4, POS, 128), BF16),
        pltpu.VMEM((4, POS, 128), BF16),
        pltpu.VMEM((4, POS, 256), BF16),
        pltpu.VMEM((4, POS, 256), BF16),
        pltpu.VMEM((POS, D), BF16),
        dma((16,)),
        dma((9,)), dma((9,)),
        dma((6,)), dma((6,)),
        dma((4, NY, 2)), dma((4, NY, 2)),
        dma((4, NZ, 2)), dma((4, NZ, 2)),
        dma((4, NY)), dma((4, NY)),
        dma((4,)), dma((4,)),
        dma((3,)), dma((3,)),
        dma((4,)), dma((4,)),
        dma((4,)), dma((4,)),
        dma((2, 3)), dma((2, 3)),
        dma((2, 3)), dma((2, 3)),
    ]
    anywhere = pl.BlockSpec(memory_space=pl.ANY)
    return pl.pallas_call(
        kernel,
        out_shape=jax.ShapeDtypeStruct((1, POS, D), BF16),
        in_specs=[anywhere] * 16,
        out_specs=anywhere,
        scratch_shapes=scratch,
        compiler_params=pltpu.CompilerParams(
            collective_id=0, has_side_effects=True, vmem_limit_bytes=48 * 1024 * 1024
        ),
        name="mixer",
    )(
        frames, norm_gain.reshape(1, -1), conv_value_w, conv_gate_w, conv_taps,
        conv_bias.reshape(1, -1), channel_gain.reshape(1, -1), channel_shift.reshape(1, -1),
        query_w, forget_w, input_w, gate_w, memory_rate.reshape(1, -1), head_gain.reshape(1, -1),
        conv_out_w, rec_out_w,
    )


def solution(mesh):
    torus = Mesh(mesh.devices.reshape(NZ, NY, NX, 2), ("z", "y", "x", "c"))
    tp, sp = ("x", "c"), ("z", "y")
    columns, rows, vector = P(None, tp), P(tp, None), P(tp)
    in_specs = (
        P(tp, sp, None), P(), columns, columns, columns, vector, vector, vector,
        columns, columns, columns, columns, vector, vector, rows, rows,
    )
    return jax.shard_map(
        local, mesh=torus, in_specs=in_specs, out_specs=P(tp, sp, None), check_vma=False
    )
```

```python
import jax
import jax.numpy as jnp
from jax import lax
from jax.experimental import pallas as pl
from jax.experimental.pallas import tpu as pltpu
from jax.sharding import Mesh
from jax.sharding import PartitionSpec as P

F32, BF16 = jnp.float32, jnp.bfloat16
MESH = pl.DeviceIdType.MESH
NZ, NY, NX = 8, 4, 4
EPS = 1e-06
POS, D, HEAD = 128, 1024, 128
TAPS, HALO = 31, 32
D_CONV = 512
SEQ_LEN = 4096
OFF = (0, -1, 1, 2)
SLOT_OF = {0: 0, 3: 1, 1: 2, 2: 3}
FG, IN, QU, GA = 0, 256, 512, 768
NT = (((1,), (1,)), ((), ()))
TN = (((0,), (0,)), ((), ()))


def dot(a, b):
    return jnp.dot(a, b, preferred_element_type=F32)


def remote(src, dst, send, recv, dev):
    return pltpu.make_async_remote_copy(
        src_ref=src, dst_ref=dst, send_sem=send, recv_sem=recv, device_id=dev, device_id_type=MESH
    )


def sigmoid(v):
    return 1.0 / (1.0 + jnp.exp(-v))


def kernel(
    frames, norm_gain, cvt, cgt, taps, cbias, cgain, cshift, qw, fw, iw, gw, rate, hgain, cow, row,
    out,
    fr_v, ng_v, taps_v, vec_v, hv_v, pk, xs, w, cwt, wc, wr,
    grown_b, inp_b, shr_b, gate_b, local_b, gt_b, cum_b,
    st_s, st_r, dec_s, dec_r, t_s, t_r, dd_s, dd_r, u_r, ud_r, h_s, h_r, c_s, c_r,
    halo_s, halo_r, ext, filt, stat_s, stat_r, ac_s, ac_r, ar_s, ar_r, out_v,
    lsem, psend, precv, gsend, grecv, r1s, r1r, r2s, r2r, x2s, x2r, h2s, h2r, r3s, r3r, hs, hr, ss, sr,
    acs, acr, ars, arr, wxs, wxr, wfs, wfr, y_in, z_in,
):
    z, y, x, c = (lax.axis_index(a) for a in ("z", "y", "x", "c"))
    partner = {"c": 1 - c}
    upper, deep = lax.div(z, 4), lax.rem(z, 4)

    def at_x(k):
        return {"x": lax.rem(x + k + NX, NX)}

    def at_y(k):
        return {"y": lax.rem(y + k, NY)}

    def signal(sem, dev):
        pl.semaphore_signal(sem, inc=1, device_id=dev, device_id_type=MESH)

    bar = pltpu.get_barrier_semaphore()
    signal(bar, partner)
    for k in (1, 2, 3):
        signal(bar, at_x(k))

    @pl.when((y == 0) & (z > 0))
    def _():
        signal(bar, {"z": z - 1, "y": NY - 1})

    loads = []

    def load(src, dst):
        copy = pltpu.make_async_copy(src, dst, lsem.at[len(loads)])
        copy.start()
        loads.append(copy)

    load(frames.at[0], fr_v)
    load(norm_gain, ng_v)
    load(taps, taps_v)
    load(cbias, vec_v.at[0])
    load(cgain, vec_v.at[1])
    load(cshift, vec_v.at[2])
    load(rate, hv_v.at[0])
    load(hgain, hv_v.at[1])
    n_small = len(loads)
    for k, ref in enumerate((fw, iw, qw, gw)):
        load(ref, w.at[:, pl.ds(256 * k, 128)])
    load(cvt, cwt.at[0, pl.ds(0, 64)])
    load(cgt, cwt.at[1, pl.ds(0, 64)])
    load(cow, wc.at[0, pl.ds(0, 64)])
    load(row, wr.at[0, pl.ds(0, 128)])
    for copy in loads[:n_small]:
        copy.wait()

    values = fr_v[...].astype(F32)
    scale = lax.rsqrt(jnp.mean(values * values, axis=-1, keepdims=True) + EPS)
    xs[0] = (values * scale * ng_v[...]).astype(BF16)
    pk[0] = jnp.zeros((40, 128), F32)
    pk[0, 0:TAPS, 0:64] = taps_v[...].astype(F32)
    for k in range(3):
        pk[0, 32 + k : 33 + k, 0:64] = vec_v[k]
    for k in range(2):
        pk[0, 35 + k : 36 + k, :] = hv_v[k]

    pl.semaphore_wait(
        bar,
        4
        + jnp.where(y > 0, 1, 0)
        + jnp.where(z > 0, 1, 0)
        + jnp.where((y == NY - 1) & (z < NZ - 1), 1, 0),
    )

    @pl.when(y < NY - 1)
    def _():
        signal(bar, {"y": y + 1})

    @pl.when(z < NZ - 1)
    def _():
        signal(bar, {"z": z + 1})

    def half(ref, s, h):
        return ref.at[s, pl.ds(64 * h, 64)]

    g = [
        remote(half(xs, 0, 0), half(xs, 1, 0), gsend.at[0], grecv.at[0], at_x(1)),
        remote(half(xs, 0, 1), half(xs, 2, 1), gsend.at[1], grecv.at[1], at_x(-1)),
        remote(half(xs, 0, 1), half(xs, 1, 1), gsend.at[2], grecv.at[2], at_x(1)),
        remote(half(xs, 0, 0), half(xs, 2, 0), gsend.at[3], grecv.at[3], at_x(-1)),
        remote(half(xs, 1, 0), half(xs, 3, 0), gsend.at[4], grecv.at[4], at_x(1)),
        remote(half(xs, 2, 1), half(xs, 3, 1), gsend.at[5], grecv.at[5], at_x(-1)),
    ]
    for copy in g[:4]:
        copy.start()

    @pl.loop(0, y)
    def _(i):
        signal(y_in, {"y": i})

    @pl.loop(0, z)
    def _(i):
        signal(z_in, {"z": i})

    p = []

    def pair(src, dst):
        copy = remote(src, dst, psend.at[len(p)], precv.at[len(p)], partner)
        copy.start()
        p.append(copy)

    for k, ref in enumerate((fw, iw)):
        pair(ref, w.at[:, pl.ds(256 * k + 128, 128)])
    pair(pk.at[0], pk.at[1])
    pair(cvt, cwt.at[0, pl.ds(64, 64)])
    pair(cgt, cwt.at[1, pl.ds(64, 64)])
    for k, ref in enumerate((qw, gw)):
        pair(ref, w.at[:, pl.ds(256 * k + 640, 128)])
    pair(cow, wc.at[0, pl.ds(64, 64)])
    pair(row, wr.at[0, pl.ds(128, 128)])

    for copy in loads[n_small:]:
        copy.wait()
    for copy in p[:3]:
        copy.wait_recv()

    def conv_rows(a, b):
        return jnp.concatenate([pk[0, a:b, 0:64], pk[1, a:b, 0:64]], axis=1)

    tap_rows = conv_rows(0, 32)
    bias_row, gain_row, shift_row = (conv_rows(32 + k, 33 + k) for k in range(3))
    rate_row = jnp.concatenate([pk[0, 35:36], pk[1, 35:36]], axis=1) / SEQ_LEN
    hgain_row = jnp.concatenate([pk[0, 36:37], pk[1, 36:37]], axis=1)

    at_t = lax.broadcasted_iota(jnp.int32, (POS, POS), 0)
    at_u = lax.broadcasted_iota(jnp.int32, (POS, POS), 1)
    causal = at_u <= at_t
    tril = jnp.where(causal, 1.0, 0.0).astype(BF16)

    started = []

    def spread(rows2):
        return jnp.concatenate(
            [jnp.broadcast_to(rows2[h : h + 1], (32, 128)) for h in range(2)], axis=0
        )

    def begin(j):
        rows = xs[j]
        forget_raw = dot(rows, w[:, FG : FG + 256]).astype(BF16).astype(F32)
        inputs = dot(rows, w[:, IN : IN + 256]).astype(BF16)
        in_gate = rate_row * sigmoid(-forget_raw)
        log_forget = jnp.log1p(-in_gate)
        hi = log_forget.astype(BF16)
        rest = log_forget - hi.astype(F32)
        mid = rest.astype(BF16)
        low = (rest - mid.astype(F32)).astype(BF16)
        cumulative = dot(tril, hi) + dot(tril, mid) + dot(tril, low)
        last = cumulative[POS - 1 : POS]
        weighted = (in_gate * jnp.exp(last - cumulative)).astype(BF16)
        for h in range(2):
            lanes = slice(128 * h, 128 * h + 128)
            state = lax.dot_general(
                inputs[:, lanes], weighted[:, lanes], TN, preferred_element_type=F32
            )
            for k in range(NY):
                st_s[j, k, 32 * h : 32 * h + 32] = state[32 * k : 32 * k + 32]
            dec_s[j, h : h + 1] = jnp.exp(last[:, lanes])
        if j == 0:

            @pl.when(y < NY - 1)
            def _():
                pl.semaphore_wait(y_in, NY - 1 - y)

        for k in (1, 2, 3):
            to = lax.rem(y + k, NY)
            a = remote(st_s.at[j, to], st_r.at[j, y], r1s.at[j, k, 0], r1r.at[j, k, 0], {"y": to})
            b = remote(dec_s.at[j], dec_r.at[j, y], r1s.at[j, k, 1], r1r.at[j, k, 1], {"y": to})
            a.start()
            b.start()
            started.extend((a, b))
        st_r[j, y] = st_s[j, y]
        dec_r[j, y] = dec_s[j]
        gt_b[j] = in_gate
        cum_b[j] = cumulative
        inp_b[j] = inputs

    def gating(j):
        rows = xs[j]
        conv_value = lax.dot_general(rows, cwt[0], NT, preferred_element_type=F32)
        conv_gate = lax.dot_general(rows, cwt[1], NT, preferred_element_type=F32)
        conv_value = conv_value.astype(BF16).astype(F32)
        conv_gate = conv_gate.astype(BF16).astype(F32)
        gated = (conv_value * sigmoid(conv_gate)).astype(BF16)
        halo_s[j] = gated[POS - HALO :]
        ext[j, HALO:] = gated.astype(F32)

        @pl.when(y < NY - 1)
        def _():
            remote(halo_s.at[j], halo_r.at[j], hs.at[j], hr.at[j], {"y": y + 1}).start()

        @pl.when((y == NY - 1) & (z < NZ - 1))
        def _():
            remote(halo_s.at[j], halo_r.at[j], hs.at[j], hr.at[j], {"z": z + 1, "y": 0}).start()

    def within(j):
        rows = xs[j]
        queries = dot(rows, w[:, QU : QU + 256]).astype(BF16).astype(F32)
        cumulative = cum_b[j]
        grown = (queries * jnp.exp(cumulative)).astype(BF16)
        shrunk = (gt_b[j] * jnp.exp(-cumulative)).astype(BF16)
        grown_b[j] = grown
        for h in range(2):
            lanes = slice(128 * h, 128 * h + 128)
            scores = lax.dot_general(
                grown[:, lanes], shrunk[:, lanes], NT, preferred_element_type=F32
            )
            scores = jnp.where(causal, scores, 0.0).astype(BF16)
            local_b[j, :, lanes] = dot(scores, inp_b[j, :, lanes])
        gate_b[j] = dot(rows, w[:, GA : GA + 256]).astype(BF16)

    def totals(j):
        for k in (1, 2, 3):
            remote(st_s.at[j, 0], st_r.at[j, 0], r1s.at[j, k, 0], r1r.at[j, k, 0], at_y(k)).wait_recv()
            remote(dec_s.at[j], dec_r.at[j, 0], r1s.at[j, k, 1], r1r.at[j, k, 1], at_y(k)).wait_recv()
        total = st_r[j, 0]
        decay = dec_r[j, 0]
        for k in (1, 2, 3):
            total = total * spread(dec_r[j, k]) + st_r[j, k]
            decay = decay * dec_r[j, k]
        t_s[j] = total.reshape(4, 16, 128)
        dd_s[j] = decay
        if j == 0:

            @pl.when(z < NZ - 1)
            def _():
                pl.semaphore_wait(z_in, NZ - 1 - z)

        @pl.loop(deep + 1, 4)
        def _(i):
            remote(t_s.at[j], t_r.at[j, deep], r2s.at[j, i, 0], r2r.at[j, deep, 0], {"z": 4 * upper + i}).start()
            remote(dd_s.at[j], dd_r.at[j, deep], r2s.at[j, i, 1], r2r.at[j, deep, 1], {"z": 4 * upper + i}).start()

        @pl.when(upper == 0)
        def _():
            @pl.loop(0, 4)
            def _(i):
                remote(t_s.at[j, i], u_r.at[j, deep], x2s.at[j, i, 0], x2r.at[j, deep, 0], {"z": 4 + i}).start()
                remote(dd_s.at[j], ud_r.at[j, deep], x2s.at[j, i, 1], x2r.at[j, deep, 1], {"z": 4 + i}).start()

    def cross(j):
        @pl.when(upper == 1)
        def _():
            first = lax.div(deep, 2)
            for i in range(4):
                remote(t_s.at[j, 0], u_r.at[j, i], x2s.at[j, i, 0], x2r.at[j, i, 0], {"z": i}).wait_recv()
                remote(dd_s.at[j], ud_r.at[j, i], x2s.at[j, i, 1], x2r.at[j, i, 1], {"z": i}).wait_recv()
            state = u_r[j, 0]
            for i in range(1, 4):
                state = state * ud_r[j, i, pl.ds(first, 1)] + u_r[j, i]
            h_s[j] = state
            for k in (1, 2, 3):
                to = lax.rem(deep + k, 4)
                remote(h_s.at[j], h_r.at[j, deep], h2s.at[j, k], h2r.at[j, k], {"z": 4 + to}).start()
            h_r[j, deep] = h_s[j]

    def carry(j):
        @pl.when(upper == 0)
        def _():
            h_r[j] = jnp.zeros((4, 16, 128), F32)

        @pl.when(upper == 1)
        def _():
            for k in (1, 2, 3):
                remote(h_s.at[j], h_r.at[j, 0], h2s.at[j, k], h2r.at[j, k], {"z": z}).wait_recv()

        def step(i, state):
            remote(t_s.at[j], t_r.at[j, i], r2s.at[j, i, 0], r2r.at[j, i, 0], {"z": i}).wait_recv()
            remote(dd_s.at[j], dd_r.at[j, i], r2s.at[j, i, 1], r2r.at[j, i, 1], {"z": i}).wait_recv()
            return state * spread(dd_r[j, i]) + t_r[j, i].reshape(64, 128)

        state = lax.fori_loop(0, deep, step, h_r[j].reshape(64, 128))
        for k in range(NY):
            c_s[j, k] = state.astype(BF16)
            if k < NY - 1:
                state = state * spread(dec_r[j, k]) + st_r[j, k]
        for k in (1, 2, 3):
            to = lax.rem(y + k, NY)
            a = remote(c_s.at[j, to], c_r.at[j, y], r3s.at[j, k], r3r.at[j, k], {"y": to})
            a.start()
            started.append(a)
        c_r[j, y] = c_s[j, y]

    def filtering(j):
        @pl.when((z > 0) | (y > 0))
        def _():
            remote(halo_s.at[j], halo_r.at[j], hs.at[j], hr.at[j], {"y": y}).wait_recv()
            ext[j, 0:HALO] = halo_r[j].astype(F32)

        @pl.when((z == 0) & (y == 0))
        def _():
            ext[j, 0:HALO] = jnp.zeros((HALO, 128), F32)

        acc = jnp.broadcast_to(bias_row, (POS, 128))
        for k in range(TAPS):
            first = HALO - (TAPS - 1) + k
            acc = acc + tap_rows[k : k + 1] * ext[j, first : first + POS]
        filt[j] = acc
        return jnp.sum(acc, axis=-1, keepdims=True), jnp.sum(acc * acc, axis=-1, keepdims=True)

    def conv_norm(j, sums, squares):
        mean = sums / D_CONV
        var = squares / D_CONV - mean * mean
        scaled = (filt[j] - mean) * lax.rsqrt(var + EPS) * gain_row + shift_row
        return (scaled * sigmoid(scaled)).astype(BF16)

    def finish(j):
        for k in (1, 2, 3):
            remote(c_s.at[j, 0], c_r.at[j, 0], r3s.at[j, k], r3r.at[j, k], at_y(k)).wait_recv()
        gate = gate_b[j].astype(F32)
        silu = gate * sigmoid(gate)
        parts = []
        for h in range(2):
            lanes = slice(128 * h, 128 * h + 128)
            low = jnp.concatenate([c_r[j, k, 32 * h : 32 * h + 32] for k in range(NY)], axis=0)
            raw = local_b[j, :, lanes] + lax.dot_general(
                grown_b[j, :, lanes], low, NT, preferred_element_type=F32
            )
            scale = lax.rsqrt(jnp.mean(raw * raw, axis=-1, keepdims=True) + EPS)
            parts.append((raw * scale * hgain_row[:, lanes] * silu[:, lanes]).astype(BF16))
        return jnp.concatenate(parts, axis=1)

    def rec_half(s, h):
        return wr.at[s, pl.ds(64 * h, 64)]

    def conv_half(s, h):
        return wc.at[s, pl.ds(32 * h, 32)]

    def own_rec(h):
        return row.at[pl.ds(64 * h, 64)]

    wx = [
        remote(own_rec(0), rec_half(1, 0), wxs.at[0], wxr.at[0], at_x(1)),
        remote(own_rec(1), rec_half(2, 1), wxs.at[1], wxr.at[1], at_x(-1)),
        remote(own_rec(1), rec_half(1, 1), wxs.at[2], wxr.at[2], at_x(1)),
        remote(own_rec(0), rec_half(2, 0), wxs.at[3], wxr.at[3], at_x(-1)),
        remote(rec_half(1, 0), rec_half(3, 0), wxs.at[4], wxr.at[4], at_x(1)),
        remote(rec_half(2, 1), rec_half(3, 1), wxs.at[5], wxr.at[5], at_x(-1)),
        remote(cow, wc.at[1, pl.ds(0, 64)], wxs.at[6], wxr.at[6], at_x(1)),
        remote(cow, wc.at[2, pl.ds(0, 64)], wxs.at[7], wxr.at[7], at_x(-1)),
        remote(conv_half(1, 0), conv_half(3, 0), wxs.at[8], wxr.at[8], at_x(1)),
        remote(conv_half(2, 1), conv_half(3, 1), wxs.at[9], wxr.at[9], at_x(-1)),
    ]
    wf = []

    def over(ref, s, size):
        n = len(wf)
        f = remote(ref.at[s, pl.ds(0, size)], ref.at[s, pl.ds(size, size)], wfs.at[n], wfr.at[n], partner)
        f.start()
        wf.append(f)

    begin(0)
    for copy in p[3:7]:
        copy.wait_recv()
    gating(0)
    g[0].wait_recv()
    g[4].start()
    g[1].wait_recv()
    g[5].start()
    for copy in wx[:4]:
        copy.start()
    within(0)
    g[2].wait_recv()
    begin(1)
    g[3].wait_recv()
    begin(2)
    totals(0)
    cross(0)
    gating(1)
    gating(2)
    g[4].wait_recv()
    g[5].wait_recv()
    begin(3)
    gating(3)
    within(1)
    totals(1)
    totals(2)
    cross(1)
    cross(2)
    within(2)
    carry(0)
    sums = [filtering(j) for j in range(4)]
    lane = lax.broadcasted_iota(jnp.int32, (POS, 128), 1)
    packed = jnp.zeros((POS, 128), F32)
    for j in range(4):
        packed = jnp.where(lane == j, sums[j][0], packed)
        packed = jnp.where(lane == 4 + j, sums[j][1], packed)
    stat_s[...] = packed.T[0:8]
    stats = []
    for n, k in enumerate((1, -1, 2)):
        s = SLOT_OF[-k % NX]
        a = remote(stat_s, stat_r.at[s], ss.at[n], sr.at[n], at_x(k))
        a.start()
        stats.append(a)
    totals(3)
    cross(3)
    wx[0].wait_recv()
    wx[4].start()
    wx[1].wait_recv()
    wx[5].start()
    for copy in wx[6:8]:
        copy.start()
    within(3)
    carry(1)
    carry(2)
    for a in stats:
        a.wait_recv()
    total = stat_s[...]
    for s in (1, 2, 3):
        got = stat_r[s]
        order = [SLOT_OF[(OFF[j] - OFF[s]) % NX] for j in range(4)]
        total = total + jnp.concatenate(
            [got[base + k : base + k + 1] for base in (0, 4) for k in order], axis=0
        )
    columns = jnp.concatenate([total, jnp.zeros((120, 128), F32)], axis=0).T
    actc = []
    for j in range(4):
        rows = conv_norm(j, columns[:, j : j + 1], columns[:, 4 + j : 5 + j])
        if j == 0:
            ac_r[0] = rows
        else:
            ac_s[j] = rows
            to = SLOT_OF[-OFF[j] % NX]
            a = remote(ac_s.at[j], ac_r.at[to], acs.at[j], acr.at[to], at_x(OFF[j]))
            a.start()
            actc.append(a)
    wx[2].wait_recv()
    over(wr, 1, 128)
    wx[3].wait_recv()
    over(wr, 2, 128)
    carry(3)
    wx[6].wait_recv()
    wx[8].start()
    wx[7].wait_recv()
    wx[9].start()
    over(wc, 1, 64)
    over(wc, 2, 64)
    actr = []
    for j in (1, 2, 0, 3):
        rows = finish(j)
        if j == 0:
            ar_r[0] = rows
        else:
            ar_s[j] = rows
            to = SLOT_OF[-OFF[j] % NX]
            a = remote(ar_s.at[j], ar_r.at[to], ars.at[j], arr.at[to], at_x(OFF[j]))
            a.start()
            actr.append(a)
    wx[4].wait_recv()
    wx[5].wait_recv()
    over(wr, 3, 128)
    wx[8].wait_recv()
    wx[9].wait_recv()
    over(wc, 3, 64)
    for copy in p[7:]:
        copy.wait_recv()
    acc = dot(ac_r[0], wc[0]) + dot(ar_r[0], wr[0])
    for f in wf:
        f.wait_recv()
    for j in (1, 2, 3):
        remote(ac_s.at[j], ac_r.at[j], acs.at[j], acr.at[j], partner).wait_recv()
        acc = acc + dot(ac_r[j], wc[j])
    for j in (1, 2, 3):
        remote(ar_s.at[j], ar_r.at[j], ars.at[j], arr.at[j], partner).wait_recv()
        acc = acc + dot(ar_r[j], wr[j])
    out_v[...] = acc.astype(BF16)
    done = pltpu.make_async_copy(out_v, out.at[0], lsem.at[0])
    done.start()
    for a in g + p + started + stats + actc + actr + wf + wx:
        a.wait_send()

    for j in range(4):
        @pl.loop(deep + 1, 4)
        def _(i):
            remote(t_s.at[j], t_r.at[j, deep], r2s.at[j, i, 0], r2r.at[j, deep, 0], {"z": z}).wait_send()
            remote(dd_s.at[j], dd_r.at[j, deep], r2s.at[j, i, 1], r2r.at[j, deep, 1], {"z": z}).wait_send()

        @pl.when(upper == 0)
        def _():
            @pl.loop(0, 4)
            def _(i):
                remote(t_s.at[j, i], u_r.at[j, deep], x2s.at[j, i, 0], x2r.at[j, deep, 0], {"z": z}).wait_send()
                remote(dd_s.at[j], ud_r.at[j, deep], x2s.at[j, i, 1], x2r.at[j, deep, 1], {"z": z}).wait_send()

        @pl.when(upper == 1)
        def _():
            for k in (1, 2, 3):
                remote(h_s.at[j], h_r.at[j, 0], h2s.at[j, k], h2r.at[j, k], {"z": z}).wait_send()

        @pl.when((y < NY - 1) | (z < NZ - 1))
        def _():
            remote(halo_s.at[j], halo_r.at[j], hs.at[j], hr.at[j], {"y": y}).wait_send()

    done.wait()


def local(
    frames, norm_gain, conv_value_w, conv_gate_w, conv_taps, conv_bias, channel_gain, channel_shift,
    query_w, forget_w, input_w, gate_w, memory_rate, head_gain, conv_out_w, rec_out_w,
):
    dma = pltpu.SemaphoreType.DMA
    scratch = [
        pltpu.VMEM((POS, D), BF16),
        pltpu.VMEM((1, D), F32),
        pltpu.VMEM((TAPS, 64), BF16),
        pltpu.VMEM((3, 1, 64), F32),
        pltpu.VMEM((2, 1, 128), F32),
        pltpu.VMEM((2, 40, 128), F32),
        pltpu.VMEM((4, POS, D), BF16),
        pltpu.VMEM((D, 1024), BF16),
        pltpu.VMEM((2, 128, D), BF16),
        pltpu.VMEM((4, 128, D), BF16),
        pltpu.VMEM((4, 256, D), BF16),
        pltpu.VMEM((4, POS, 256), BF16),
        pltpu.VMEM((4, POS, 256), BF16),
        pltpu.VMEM((4, POS, 256), BF16),
        pltpu.VMEM((4, POS, 256), BF16),
        pltpu.VMEM((4, POS, 256), F32),
        pltpu.VMEM((4, POS, 256), F32),
        pltpu.VMEM((4, POS, 256), F32),
        pltpu.VMEM((4, NY, 64, 128), F32),
        pltpu.VMEM((4, NY, 64, 128), F32),
        pltpu.VMEM((4, 2, 128), F32),
        pltpu.VMEM((4, NY, 2, 128), F32),
        pltpu.VMEM((4, 4, 16, 128), F32),
        pltpu.VMEM((4, 4, 4, 16, 128), F32),
        pltpu.VMEM((4, 2, 128), F32),
        pltpu.VMEM((4, 4, 2, 128), F32),
        pltpu.VMEM((4, 4, 16, 128), F32),
        pltpu.VMEM((4, 4, 2, 128), F32),
        pltpu.VMEM((4, 16, 128), F32),
        pltpu.VMEM((4, 4, 16, 128), F32),
        pltpu.VMEM((4, NY, 64, 128), BF16),
        pltpu.VMEM((4, NY, 64, 128), BF16),
        pltpu.VMEM((4, HALO, 128), BF16),
        pltpu.VMEM((4, HALO, 128), BF16),
        pltpu.VMEM((4, HALO + POS, 128), F32),
        pltpu.VMEM((4, POS, 128), F32),
        pltpu.VMEM((8, 128), F32),
        pltpu.VMEM((4, 8, 128), F32),
        pltpu.VMEM((4, POS, 128), BF16),
        pltpu.VMEM((4, POS, 128), BF16),
        pltpu.VMEM((4, POS, 256), BF16),
        pltpu.VMEM((4, POS, 256), BF16),
        pltpu.VMEM((POS, D), BF16),
        dma((16,)),
        dma((9,)), dma((9,)),
        dma((6,)), dma((6,)),
        dma((4, NY, 2)), dma((4, NY, 2)),
        dma((4, 4, 2)), dma((4, 4, 2)),
        dma((4, 4, 2)), dma((4, 4, 2)),
        dma((4, 4)), dma((4, 4)),
        dma((4, NY)), dma((4, NY)),
        dma((4,)), dma((4,)),
        dma((3,)), dma((3,)),
        dma((4,)), dma((4,)),
        dma((4,)), dma((4,)),
        dma((10,)), dma((10,)),
        dma((6,)), dma((6,)),
        pltpu.SemaphoreType.REGULAR, pltpu.SemaphoreType.REGULAR,
    ]
    anywhere = pl.BlockSpec(memory_space=pltpu.HBM)
    return pl.pallas_call(
        kernel,
        out_shape=jax.ShapeDtypeStruct((1, POS, D), BF16),
        in_specs=[anywhere] * 16,
        out_specs=anywhere,
        scratch_shapes=scratch,
        compiler_params=pltpu.CompilerParams(
            collective_id=0, has_side_effects=True, vmem_limit_bytes=67043328
        ),
        name="mixer",
    )(
        frames, norm_gain.reshape(1, -1), conv_value_w.T, conv_gate_w.T, conv_taps,
        conv_bias.reshape(1, -1), channel_gain.reshape(1, -1), channel_shift.reshape(1, -1),
        query_w, forget_w, input_w, gate_w, memory_rate.reshape(1, -1), head_gain.reshape(1, -1),
        conv_out_w, rec_out_w,
    )


def solution(mesh):
    torus = Mesh(mesh.devices.reshape(NZ, NY, NX, 2), ("z", "y", "x", "c"))
    tp, sp = ("x", "c"), ("z", "y")
    columns, rows, vector = P(None, tp), P(tp, None), P(tp)
    in_specs = (
        P(tp, sp, None), P(), columns, columns, columns, vector, vector, vector,
        columns, columns, columns, columns, vector, vector, rows, rows,
    )
    return jax.shard_map(
        local, mesh=torus, in_specs=in_specs, out_specs=P(tp, sp, None), check_vma=False
    )
```

```python
import jax
import jax.numpy as jnp
from jax import lax
from jax.experimental import pallas as pl
from jax.experimental.pallas import tpu as pltpu
from jax.sharding import Mesh
from jax.sharding import PartitionSpec as P

F32, BF16 = jnp.float32, jnp.bfloat16
MESH = pl.DeviceIdType.MESH
NZ, NY, NX = 8, 4, 4
EPS = 1e-06
POS, D, HEAD = 128, 1024, 128
TAPS, HALO = 31, 32
D_CONV = 512
SEQ_LEN = 4096
OFF = (0, -1, 1, 2)
SLOT_OF = {0: 0, 3: 1, 1: 2, 2: 3}
FG, IN, QU, GA = 0, 256, 512, 768
NT = (((1,), (1,)), ((), ()))
TN = (((0,), (0,)), ((), ()))


def dot(a, b):
    return jnp.dot(a, b, preferred_element_type=F32)


def remote(src, dst, send, recv, dev):
    return pltpu.make_async_remote_copy(
        src_ref=src, dst_ref=dst, send_sem=send, recv_sem=recv, device_id=dev, device_id_type=MESH
    )


def sigmoid(v):
    return 1.0 / (1.0 + jnp.exp(-v))


def kernel(
    frames, norm_gain, cvt, cgt, taps, cbias, cgain, cshift, qw, fw, iw, gw, rate, hgain, cow, row,
    out,
    fr_v, ng_v, taps_v, vec_v, hv_v, pk, xs, w, cwt, wc, wr,
    grown_b, inp_b, gate_b, local_b, gt_b, cum_b,
    st_s, st_r, dec_s, dec_r, t_s, t_r, dd_s, dd_r, u_s, u_r, e_s, e_r, c_s, c_r,
    halo_s, halo_r, ext, filt, stat_s, stat_r, ac_s, ac_r, ar_s, ar_r,
    lsem, psend, precv, gsend, grecv, r1s, r1r, r2s, r2r, x2s, x2r, h2s, h2r, r3s, r3r, hs, hr,
    ss, sr, acs, acr, ars, arr, wxs, wxr, wfs, wfr, y_in, z_in,
):
    z, y, x, c = (lax.axis_index(a) for a in ("z", "y", "x", "c"))
    partner = {"c": 1 - c}
    upper, deep = lax.div(z, 4), lax.rem(z, 4)

    def at_x(k):
        return {"x": lax.rem(x + k + NX, NX)}

    def signal(sem, dev):
        pl.semaphore_signal(sem, inc=1, device_id=dev, device_id_type=MESH)

    def arrived(ref, sem):
        remote(ref, ref, sem, sem, partner).wait_recv()

    def sent(ref, sem):
        remote(ref, ref, sem, sem, partner).wait_send()

    bar = pltpu.get_barrier_semaphore()
    signal(bar, partner)
    for k in (1, 2, 3):
        signal(bar, at_x(k))

    @pl.loop(y + 1, NY)
    def _(i):
        signal(bar, {"y": i})

    @pl.loop(z + 1, NZ)
    def _(i):
        signal(bar, {"z": i})

    @pl.when((y == 0) & (z > 0))
    def _():
        signal(bar, {"z": z - 1, "y": NY - 1})

    loaded = []

    def load(src, dst, n):
        pltpu.make_async_copy(src, dst, lsem.at[n]).start()

    def wait_load(ref, n):
        pltpu.make_async_copy(ref, ref, lsem.at[n]).wait()

    load(frames.at[0], fr_v, 0)
    load(norm_gain, ng_v, 1)
    small = ((taps, taps_v), (cbias, vec_v.at[0]), (cgain, vec_v.at[1]), (cshift, vec_v.at[2]), (rate, hv_v.at[0]), (hgain, hv_v.at[1]))
    for n, (src, dst) in enumerate(small):
        load(src, dst, 2 + n)
    load(fw, w.at[:, pl.ds(FG, 128)], 8)
    load(iw, w.at[:, pl.ds(IN, 128)], 8)
    load(qw, w.at[:, pl.ds(QU, 128)], 9)
    load(gw, w.at[:, pl.ds(GA, 128)], 9)
    load(cvt, cwt.at[0, pl.ds(0, 64)], 10)
    load(cgt, cwt.at[1, pl.ds(0, 64)], 10)
    load(cow, wc.at[0, pl.ds(0, 64)], 11)
    load(row, wr.at[0, pl.ds(0, 128)], 12)
    wait_load(fr_v, 0)
    wait_load(ng_v, 1)

    values = fr_v[...].astype(F32)
    scale = lax.rsqrt(jnp.mean(values * values, axis=-1, keepdims=True) + EPS)
    xs[0] = (values * scale * ng_v[...]).astype(BF16)
    for n, (src, dst) in enumerate(small):
        wait_load(dst, 2 + n)
    pk[0] = jnp.zeros((40, 128), F32)
    pk[0, 0:TAPS, 0:64] = taps_v[...].astype(F32)
    for k in range(3):
        pk[0, 32 + k : 33 + k, 0:64] = vec_v[k]
    for k in range(2):
        pk[0, 35 + k : 36 + k, :] = hv_v[k]

    pl.semaphore_wait(
        bar,
        4 + y + z + jnp.where((y == NY - 1) & (z < NZ - 1), 1, 0),
    )

    def half(ref, s, h):
        return ref.at[s, pl.ds(64 * h, 64)]

    g = [
        remote(half(xs, 0, 0), half(xs, 1, 0), gsend, grecv.at[0], at_x(1)),
        remote(half(xs, 0, 1), half(xs, 2, 1), gsend, grecv.at[1], at_x(-1)),
        remote(half(xs, 0, 1), half(xs, 1, 1), gsend, grecv.at[2], at_x(1)),
        remote(half(xs, 0, 0), half(xs, 2, 0), gsend, grecv.at[3], at_x(-1)),
        remote(half(xs, 1, 0), half(xs, 3, 0), gsend, grecv.at[4], at_x(1)),
        remote(half(xs, 2, 1), half(xs, 3, 1), gsend, grecv.at[5], at_x(-1)),
    ]
    for copy in g[:4]:
        copy.start()

    @pl.loop(0, y)
    def _(i):
        signal(y_in, {"y": i})

    @pl.loop(4 * upper, z)
    def _(i):
        signal(z_in, {"z": i})

    @pl.when(upper == 1)
    def _():
        signal(z_in, {"z": z - 4})

    remote(fw, w.at[:, pl.ds(FG + 128, 128)], psend.at[0], precv.at[0], partner).start()
    remote(iw, w.at[:, pl.ds(IN + 128, 128)], psend.at[0], precv.at[0], partner).start()
    remote(pk.at[0], pk.at[1], psend.at[2], precv.at[3], partner).start()
    remote(cvt, cwt.at[0, pl.ds(64, 64)], psend.at[1], precv.at[2], partner).start()
    remote(cgt, cwt.at[1, pl.ds(64, 64)], psend.at[1], precv.at[2], partner).start()
    remote(qw, w.at[:, pl.ds(QU + 128, 128)], psend.at[0], precv.at[1], partner).start()
    remote(gw, w.at[:, pl.ds(GA + 128, 128)], psend.at[0], precv.at[1], partner).start()
    remote(cow, wc.at[0, pl.ds(64, 64)], psend.at[3], precv.at[4], partner).start()
    remote(row, wr.at[0, pl.ds(128, 128)], psend.at[4], precv.at[5], partner).start()

    wait_load(w.at[:, pl.ds(0, 256)], 8)
    wait_load(w.at[:, pl.ds(0, 256)], 9)
    wait_load(cwt.at[0], 10)
    arrived(w.at[:, pl.ds(0, 256)], precv.at[0])
    arrived(pk.at[1], precv.at[3])

    def conv_rows(a, b):
        return jnp.concatenate([pk[0, a:b, 0:64], pk[1, a:b, 0:64]], axis=1)

    tap_rows = conv_rows(0, 32)
    bias_row, gain_row, shift_row = (conv_rows(32 + k, 33 + k) for k in range(3))
    rate_row = jnp.concatenate([pk[0, 35:36], pk[1, 35:36]], axis=1) / SEQ_LEN
    hgain_row = jnp.concatenate([pk[0, 36:37], pk[1, 36:37]], axis=1)

    at_t = lax.broadcasted_iota(jnp.int32, (POS, POS), 0)
    at_u = lax.broadcasted_iota(jnp.int32, (POS, POS), 1)
    causal = at_u <= at_t
    tril = jnp.where(causal, 1.0, 0.0).astype(BF16)

    def spread(rows2):
        return jnp.concatenate(
            [jnp.broadcast_to(rows2[h : h + 1], (32, 128)) for h in range(2)], axis=0
        )

    def begin(j):
        rows = xs[j]
        forget_raw = dot(rows, w[:, FG : FG + 256]).astype(BF16).astype(F32)
        inputs = dot(rows, w[:, IN : IN + 256]).astype(BF16)
        in_gate = rate_row * sigmoid(-forget_raw)
        log_forget = jnp.log1p(-in_gate)
        hi = log_forget.astype(BF16)
        rest = log_forget - hi.astype(F32)
        mid = rest.astype(BF16)
        low = (rest - mid.astype(F32)).astype(BF16)
        cumulative = dot(tril, hi) + dot(tril, mid) + dot(tril, low)
        last = cumulative[POS - 1 : POS]
        weighted = (in_gate * jnp.exp(last - cumulative)).astype(BF16)
        for h in range(2):
            lanes = slice(128 * h, 128 * h + 128)
            state = lax.dot_general(
                inputs[:, lanes], weighted[:, lanes], TN, preferred_element_type=F32
            )
            for k in range(NY):
                st_s[j, k, 32 * h : 32 * h + 32] = state[32 * k : 32 * k + 32]
            dec_s[j, h : h + 1] = jnp.exp(last[:, lanes])
        gt_b[j] = in_gate
        cum_b[j] = cumulative
        inp_b[j] = inputs

    def deal(j):
        for k in (2, 1, 3):
            to = lax.rem(y + k, NY)
            remote(st_s.at[j, to], st_r.at[j, y], r1s.at[0], r1r.at[j, 0], {"y": to}).start()
            remote(dec_s.at[j], dec_r.at[j, y], r1s.at[1], r1r.at[j, 1], {"y": to}).start()
        st_r[j, y] = st_s[j, y]
        dec_r[j, y] = dec_s[j]

    def gating(j):
        rows = xs[j]
        conv_value = lax.dot_general(rows, cwt[0], NT, preferred_element_type=F32)
        conv_gate = lax.dot_general(rows, cwt[1], NT, preferred_element_type=F32)
        conv_value = conv_value.astype(BF16).astype(F32)
        conv_gate = conv_gate.astype(BF16).astype(F32)
        gated = (conv_value * sigmoid(conv_gate)).astype(BF16)
        halo_s[j] = gated[POS - HALO :]
        ext[j, HALO:] = gated.astype(F32)

    def pass_on(j):
        @pl.when(y < NY - 1)
        def _():
            remote(halo_s.at[j], halo_r.at[j], hs, hr.at[j], {"y": y + 1}).start()

        @pl.when((y == NY - 1) & (z < NZ - 1))
        def _():
            remote(halo_s.at[j], halo_r.at[j], hs, hr.at[j], {"z": z + 1, "y": 0}).start()

    def within(j):
        rows = xs[j]
        queries = dot(rows, w[:, QU : QU + 256]).astype(BF16).astype(F32)
        cumulative = cum_b[j]
        grown = (queries * jnp.exp(cumulative)).astype(BF16)
        shrunk = (gt_b[j] * jnp.exp(-cumulative)).astype(BF16)
        grown_b[j] = grown
        for h in range(2):
            lanes = slice(128 * h, 128 * h + 128)
            scores = lax.dot_general(
                grown[:, lanes], shrunk[:, lanes], NT, preferred_element_type=F32
            )
            scores = jnp.where(causal, scores, 0.0).astype(BF16)
            local_b[j, :, lanes] = dot(scores, inp_b[j, :, lanes])
        gate_b[j] = dot(rows, w[:, GA : GA + 256]).astype(BF16)

    def totals(j):
        arrived(st_r.at[j, pl.ds(0, 3)], r1r.at[j, 0])
        arrived(dec_r.at[j, pl.ds(0, 3)], r1r.at[j, 1])
        total = st_r[j, 0]
        decay = dec_r[j, 0]
        for k in (1, 2, 3):
            total = total * spread(dec_r[j, k]) + st_r[j, k]
            decay = decay * dec_r[j, k]
        t_s[j] = total.reshape(4, 16, 128)
        dd_s[j] = decay
        for k in (2, 1, 3):
            to = lax.rem(deep + k, 4)
            dev = {"z": 4 * upper + to}
            remote(t_s.at[j, to], t_r.at[j, deep], r2s.at[0], r2r.at[j, 0], dev).start()
            remote(dd_s.at[j], dd_r.at[j, deep], r2s.at[1], r2r.at[j, 1], dev).start()
        t_r[j, deep] = t_s[j, deep]
        dd_r[j, deep] = dd_s[j]

    def fold(j):
        head = lax.div(deep, 2)
        arrived(t_r.at[j, pl.ds(0, 3)], r2r.at[j, 0])
        arrived(dd_r.at[j, pl.ds(0, 3)], r2r.at[j, 1])

        @pl.when(upper == 0)
        def _():
            u_r[j] = jnp.zeros((16, 128), F32)

        @pl.when(upper == 1)
        def _():
            arrived(u_r.at[j], x2r.at[j])

        state = u_r[j]
        for i in range(4):
            e_s[j, i] = state
            state = state * dd_r[j, i, pl.ds(head, 1)] + t_r[j, i]
        u_s[j] = state

        @pl.when(upper == 0)
        def _():
            remote(u_s.at[j], u_r.at[j], x2s, x2r.at[j], {"z": z + 4}).start()

        for k in (2, 1, 3):
            to = lax.rem(deep + k, 4)
            remote(e_s.at[j, to], e_r.at[j, deep], h2s, h2r.at[j], {"z": 4 * upper + to}).start()
        e_r[j, deep] = e_s[j, deep]

    def carry(j):
        arrived(e_r.at[j, pl.ds(0, 3)], h2r.at[j])
        state = e_r[j].reshape(64, 128)
        for k in range(NY):
            c_s[j, k] = state.astype(BF16)
            if k < NY - 1:
                state = state * spread(dec_r[j, k]) + st_r[j, k]
        for k in (2, 1, 3):
            to = lax.rem(y + k, NY)
            remote(c_s.at[j, to], c_r.at[j, y], r3s, r3r.at[j], {"y": to}).start()
        c_r[j, y] = c_s[j, y]

    def filtering(j):
        @pl.when((z > 0) | (y > 0))
        def _():
            arrived(halo_r.at[j], hr.at[j])
            ext[j, 0:HALO] = halo_r[j].astype(F32)

        @pl.when((z == 0) & (y == 0))
        def _():
            ext[j, 0:HALO] = jnp.zeros((HALO, 128), F32)

        acc = jnp.broadcast_to(bias_row, (POS, 128))
        for k in range(TAPS):
            first = HALO - (TAPS - 1) + k
            acc = acc + tap_rows[k : k + 1] * ext[j, first : first + POS]
        filt[j] = acc
        return jnp.sum(acc, axis=-1, keepdims=True), jnp.sum(acc * acc, axis=-1, keepdims=True)

    def conv_norm(j, sums, squares):
        mean = sums / D_CONV
        var = squares / D_CONV - mean * mean
        scaled = (filt[j] - mean) * lax.rsqrt(var + EPS) * gain_row + shift_row
        return (scaled * sigmoid(scaled)).astype(BF16)

    def finish(j):
        arrived(c_r.at[j, pl.ds(0, 3)], r3r.at[j])
        gate = gate_b[j].astype(F32)
        silu = gate * sigmoid(gate)
        parts = []
        for h in range(2):
            lanes = slice(128 * h, 128 * h + 128)
            low = jnp.concatenate([c_r[j, k, 32 * h : 32 * h + 32] for k in range(NY)], axis=0)
            raw = local_b[j, :, lanes] + lax.dot_general(
                grown_b[j, :, lanes], low, NT, preferred_element_type=F32
            )
            scale = lax.rsqrt(jnp.mean(raw * raw, axis=-1, keepdims=True) + EPS)
            parts.append((raw * scale * hgain_row[:, lanes] * silu[:, lanes]).astype(BF16))
        return jnp.concatenate(parts, axis=1)

    def rec_half(s, h):
        return wr.at[s, pl.ds(64 * h, 64)]

    def conv_half(s, h):
        return wc.at[s, pl.ds(32 * h, 32)]

    def own(h):
        return row.at[pl.ds(64 * h, 64)], cow.at[pl.ds(32 * h, 32)]

    rs, cs = wxs.at[0], wxs.at[1]

    def send_own(k, h):
        s = SLOT_OF[-k % NX]
        a, b = own(h)
        remote(a, rec_half(s, h), rs, wxr.at[s, h, 0], at_x(k)).start()
        remote(b, conv_half(s, h), cs, wxr.at[s, h, 1], at_x(k)).start()

    def send_on(k, h):
        s = SLOT_OF[-k % NX]
        arrived(rec_half(s, h), wxr.at[s, h, 0])
        remote(rec_half(s, h), rec_half(3, h), rs, wxr.at[3, h, 0], at_x(k)).start()
        arrived(conv_half(s, h), wxr.at[s, h, 1])
        remote(conv_half(s, h), conv_half(3, h), cs, wxr.at[3, h, 1], at_x(k)).start()

    def over(s, halves):
        for h in halves:
            arrived(rec_half(s, h), wxr.at[s, h, 0])
            arrived(conv_half(s, h), wxr.at[s, h, 1])
        remote(wr.at[s, pl.ds(0, 128)], wr.at[s, pl.ds(128, 128)], wfs.at[0], wfr.at[0], partner).start()
        remote(wc.at[s, pl.ds(0, 64)], wc.at[s, pl.ds(64, 64)], wfs.at[1], wfr.at[1], partner).start()

    def spread_out(j, rows):
        if j == 0:
            ar_r[3] = rows
        else:
            ar_s[j - 1] = rows
            to = SLOT_OF[-OFF[j] % NX] - 1
            remote(ar_s.at[j - 1], ar_r.at[to], ars, arr.at[to], at_x(OFF[j])).start()

    begin(0)
    arrived(cwt.at[0], precv.at[2])
    gating(0)

    @pl.when(y < NY - 1)
    def _():
        pl.semaphore_wait(y_in, NY - 1 - y)

    deal(0)
    pass_on(0)
    arrived(w.at[:, pl.ds(0, 256)], precv.at[1])
    within(0)
    g[0].wait_recv()
    g[4].start()
    g[1].wait_recv()
    g[5].start()
    send_own(1, 0)
    send_own(-1, 1)
    send_own(1, 1)
    send_own(-1, 0)
    g[2].wait_recv()
    begin(1)
    deal(1)
    g[3].wait_recv()
    begin(2)
    deal(2)

    @pl.when(z < NZ - 1)
    def _():
        pl.semaphore_wait(z_in, 4 - deep - upper)

    totals(0)
    g[4].wait_recv()
    g[5].wait_recv()
    begin(3)
    deal(3)
    gating(1)
    pass_on(1)
    gating(2)
    pass_on(2)
    gating(3)
    pass_on(3)
    totals(1)
    totals(2)
    fold(0)
    within(1)
    totals(3)
    sums = [filtering(j) for j in range(4)]
    lane = lax.broadcasted_iota(jnp.int32, (POS, 128), 1)
    packed = jnp.zeros((POS, 128), F32)
    for j in range(4):
        packed = jnp.where(lane == j, sums[j][0], packed)
        packed = jnp.where(lane == 4 + j, sums[j][1], packed)
    stat_s[...] = packed.T[0:8]
    for k in (1, -1, 2):
        remote(stat_s, stat_r.at[SLOT_OF[-k % NX] - 1], ss, sr, at_x(k)).start()
    within(2)
    fold(1)
    fold(2)
    send_on(1, 0)
    send_on(-1, 1)
    within(3)
    carry(0)
    fold(3)
    arrived(stat_r, sr)
    total = stat_s[...]
    for s in (1, 2, 3):
        got = stat_r[s - 1]
        order = [SLOT_OF[(OFF[j] - OFF[s]) % NX] for j in range(4)]
        total = total + jnp.concatenate(
            [got[base + k : base + k + 1] for base in (0, 4) for k in order], axis=0
        )
    columns = jnp.concatenate([total, jnp.zeros((120, 128), F32)], axis=0).T
    for j in range(4):
        rows = conv_norm(j, columns[:, j : j + 1], columns[:, 4 + j : 5 + j])
        if j == 0:
            ac_r[3] = rows
        else:
            ac_s[j - 1] = rows
            remote(ac_s.at[j - 1], ac_r.at[SLOT_OF[-OFF[j] % NX] - 1], acs, acr, at_x(OFF[j])).start()
    carry(1)
    carry(2)
    over(1, (1,))
    over(2, (0,))
    carry(3)
    spread_out(0, finish(0))
    for j in (1, 2):
        rows = finish(j)
        spread_out(j, rows)
    over(3, (0, 1))
    rows = finish(3)
    spread_out(3, rows)
    wait_load(wc.at[0, pl.ds(0, 64)], 11)
    wait_load(wr.at[0, pl.ds(0, 128)], 12)
    arrived(wc.at[0, pl.ds(0, 64)], precv.at[4])
    arrived(wr.at[0, pl.ds(0, 128)], precv.at[5])
    acc = dot(ac_r[3], wc[0]) + dot(ar_r[3], wr[0])
    arrived(wc.at[pl.ds(0, 3), pl.ds(0, 64)], wfr.at[1])
    arrived(ac_r.at[pl.ds(0, 3)], acr)
    for j in (1, 2, 3):
        acc = acc + dot(ac_r[j - 1], wc[j])
    arrived(wr.at[pl.ds(0, 3), pl.ds(0, 128)], wfr.at[0])
    for j in (1, 2, 3):
        arrived(ar_r.at[j - 1], arr.at[j - 1])
        acc = acc + dot(ar_r[j - 1], wr[j])
    out[0] = acc.astype(BF16)

    sent(w.at[:, pl.ds(0, 512)], psend.at[0])
    sent(cwt.at[0], psend.at[1])
    sent(pk.at[0], psend.at[2])
    sent(wc.at[0, pl.ds(0, 64)], psend.at[3])
    sent(wr.at[0, pl.ds(0, 128)], psend.at[4])
    sent(xs.at[pl.ds(0, 3)], gsend)
    sent(st_s.at[pl.ds(0, 3)], r1s.at[0])
    sent(dec_r.at[pl.ds(0, 3)], r1s.at[1])
    sent(t_r.at[pl.ds(0, 3)], r2s.at[0])
    sent(dd_r.at[pl.ds(0, 3)], r2s.at[1])
    sent(e_r.at[pl.ds(0, 3)], h2s)

    @pl.when(upper == 0)
    def _():
        sent(u_s, x2s)

    sent(c_r.at[pl.ds(0, 3)], r3s)

    @pl.when((y < NY - 1) | (z < NZ - 1))
    def _():
        sent(halo_s, hs)

    sent(stat_r, ss)
    sent(ac_s, acs)
    sent(ar_s, ars)
    sent(wr.at[pl.ds(0, 3), pl.ds(0, 128)], wxs.at[0])
    sent(wc.at[pl.ds(0, 3), pl.ds(0, 64)], wxs.at[1])
    sent(wr.at[pl.ds(0, 3), pl.ds(0, 128)], wfs.at[0])
    sent(wc.at[pl.ds(0, 3), pl.ds(0, 64)], wfs.at[1])


def local(
    frames, norm_gain, conv_value_w, conv_gate_w, conv_taps, conv_bias, channel_gain, channel_shift,
    query_w, forget_w, input_w, gate_w, memory_rate, head_gain, conv_out_w, rec_out_w,
):
    dma = pltpu.SemaphoreType.DMA
    scratch = [
        pltpu.VMEM((POS, D), BF16),
        pltpu.VMEM((1, D), F32),
        pltpu.VMEM((TAPS, 64), BF16),
        pltpu.VMEM((3, 1, 64), F32),
        pltpu.VMEM((2, 1, 128), F32),
        pltpu.VMEM((2, 40, 128), F32),
        pltpu.VMEM((4, POS, D), BF16),
        pltpu.VMEM((D, 1024), BF16),
        pltpu.VMEM((2, 128, D), BF16),
        pltpu.VMEM((4, 128, D), BF16),
        pltpu.VMEM((4, 256, D), BF16),
        pltpu.VMEM((4, POS, 256), BF16),
        pltpu.VMEM((4, POS, 256), BF16),
        pltpu.VMEM((4, POS, 256), BF16),
        pltpu.VMEM((4, POS, 256), F32),
        pltpu.VMEM((4, POS, 256), F32),
        pltpu.VMEM((4, POS, 256), F32),
        pltpu.VMEM((4, NY, 64, 128), F32),
        pltpu.VMEM((4, NY, 64, 128), F32),
        pltpu.VMEM((4, 2, 128), F32),
        pltpu.VMEM((4, NY, 2, 128), F32),
        pltpu.VMEM((4, 4, 16, 128), F32),
        pltpu.VMEM((4, 4, 16, 128), F32),
        pltpu.VMEM((4, 2, 128), F32),
        pltpu.VMEM((4, 4, 2, 128), F32),
        pltpu.VMEM((4, 16, 128), F32),
        pltpu.VMEM((4, 16, 128), F32),
        pltpu.VMEM((4, 4, 16, 128), F32),
        pltpu.VMEM((4, 4, 16, 128), F32),
        pltpu.VMEM((4, NY, 64, 128), BF16),
        pltpu.VMEM((4, NY, 64, 128), BF16),
        pltpu.VMEM((4, HALO, 128), BF16),
        pltpu.VMEM((4, HALO, 128), BF16),
        pltpu.VMEM((4, HALO + POS, 128), F32),
        pltpu.VMEM((4, POS, 128), F32),
        pltpu.VMEM((8, 128), F32),
        pltpu.VMEM((3, 8, 128), F32),
        pltpu.VMEM((3, POS, 128), BF16),
        pltpu.VMEM((4, POS, 128), BF16),
        pltpu.VMEM((3, POS, 256), BF16),
        pltpu.VMEM((4, POS, 256), BF16),
        dma((13,)),
        dma((5,)), dma((6,)),
        dma(()), dma((6,)),
        dma((2,)), dma((4, 2)),
        dma((2,)), dma((4, 2)),
        dma(()), dma((4,)),
        dma(()), dma((4,)),
        dma(()), dma((4,)),
        dma(()), dma((4,)),
        dma(()), dma(()),
        dma(()), dma(()),
        dma(()), dma((3,)),
        dma((2,)), dma((4, 2, 2)),
        dma((2,)), dma((2,)),
        pltpu.SemaphoreType.REGULAR, pltpu.SemaphoreType.REGULAR,
    ]
    anywhere = pl.BlockSpec(memory_space=pltpu.HBM)
    return pl.pallas_call(
        kernel,
        out_shape=jax.ShapeDtypeStruct((1, POS, D), BF16),
        in_specs=[anywhere] * 16,
        out_specs=pl.BlockSpec(memory_space=pltpu.VMEM),
        scratch_shapes=scratch,
        compiler_params=pltpu.CompilerParams(
            collective_id=0, has_side_effects=True, vmem_limit_bytes=67043328 - 270 * 1024
        ),
        name="mixer",
    )(
        frames, norm_gain.reshape(1, -1), conv_value_w.T, conv_gate_w.T, conv_taps,
        conv_bias.reshape(1, -1), channel_gain.reshape(1, -1), channel_shift.reshape(1, -1),
        query_w, forget_w, input_w, gate_w, memory_rate.reshape(1, -1), head_gain.reshape(1, -1),
        conv_out_w, rec_out_w,
    )


def solution(mesh):
    torus = Mesh(mesh.devices.reshape(NZ, NY, NX, 2), ("z", "y", "x", "c"))
    tp, sp = ("x", "c"), ("z", "y")
    columns, rows, vector = P(None, tp), P(tp, None), P(tp)
    in_specs = (
        P(tp, sp, None), P(), columns, columns, columns, vector, vector, vector,
        columns, columns, columns, columns, vector, vector, rows, rows,
    )
    return jax.shard_map(
        local, mesh=torus, in_specs=in_specs, out_specs=P(tp, sp, None), check_vma=False
    )
```

```python
import jax
import jax.numpy as jnp
from jax import lax
from jax.experimental import pallas as pl
from jax.experimental.pallas import tpu as pltpu
from jax.sharding import Mesh
from jax.sharding import PartitionSpec as P

F32, BF16 = jnp.float32, jnp.bfloat16
MESH = pl.DeviceIdType.MESH
NZ, NY, NX = 8, 4, 4
EPS = 1e-06
POS, D, HEAD = 128, 1024, 128
TAPS, HALO = 31, 32
D_CONV = 512
SEQ_LEN = 4096
OFF = (0, -1, 1, 2)
SLOT_OF = {0: 0, 3: 1, 1: 2, 2: 3}
FG, IN, QU, GA = 0, 256, 512, 768
NT = (((1,), (1,)), ((), ()))
TN = (((0,), (0,)), ((), ()))


def dot(a, b):
    return jnp.dot(a, b, preferred_element_type=F32)


def remote(src, dst, send, recv, dev):
    return pltpu.make_async_remote_copy(
        src_ref=src, dst_ref=dst, send_sem=send, recv_sem=recv, device_id=dev, device_id_type=MESH
    )


def sigmoid(v):
    return 1.0 / (1.0 + jnp.exp(-v))


def kernel(
    frames, norm_gain, cvt, cgt, taps, cbias, cgain, cshift, qw, fw, iw, gw, rate, hgain, cow, row,
    out,
    fr_v, ng_v, taps_v, vec_v, hv_v, pk, xs, w, cwt, wc, wr,
    grown_b, inp_b, gate_b, local_b, gt_b, cum_b,
    st_s, st_r, dec_s, dec_r, t_s, t_r, dd_s, dd_r, c_s, c_r,
    halo_s, halo_r, ext, filt, stat_s, stat_r, ac_s, ac_r, ar_s, ar_r,
    lsem, psend, precv, gsend, grecv, r1s, r1r, r2s, r2r, r3s, r3r, hs, hr,
    ss, sr, acs, acr, ars, arr, wxs, wxr, wfs, wfr, y_in, z_in,
):
    z, y, x, c = (lax.axis_index(a) for a in ("z", "y", "x", "c"))
    partner = {"c": 1 - c}
    pair, odd = lax.div(z, 2), lax.rem(z, 2)
    me = odd * NY + y

    def mate(flip, k):
        z2, y2 = lax.rem(odd + flip, 2), lax.rem(y + k, NY)
        return {"z": 2 * pair + z2, "y": y2}, z2 * NY + y2

    mates = [mate(*m) for m in ((1, 2), (1, 1), (1, 3), (1, 0), (0, 2), (0, 1), (0, 3))]

    def at_x(k):
        return {"x": lax.rem(x + k + NX, NX)}

    def signal(sem, dev):
        pl.semaphore_signal(sem, inc=1, device_id=dev, device_id_type=MESH)

    def arrived(ref, sem):
        remote(ref, ref, sem, sem, partner).wait_recv()

    def sent(ref, sem):
        remote(ref, ref, sem, sem, partner).wait_send()

    bar = pltpu.get_barrier_semaphore()
    signal(bar, partner)
    for k in (1, 2, 3):
        signal(bar, at_x(k))

    def rank(number):
        return 2 * lax.min(lax.rem(number, NY), 2) + 2 * lax.div(number, NY)

    ahead = 0
    for dev, number in mates:
        ahead = ahead + jnp.where(rank(number) <= rank(me), 1, 0)

        @pl.when(rank(number) >= rank(me))
        def _():
            signal(bar, dev)

    @pl.loop(pair + 1, 4)
    def _(i):
        signal(bar, {"z": 2 * i + odd})

    @pl.when((y == 0) & (odd == 0) & (z > 0))
    def _():
        signal(bar, {"z": z - 1, "y": NY - 1})

    loaded = []

    def load(src, dst, n):
        pltpu.make_async_copy(src, dst, lsem.at[n]).start()

    def wait_load(ref, n):
        pltpu.make_async_copy(ref, ref, lsem.at[n]).wait()

    load(frames.at[0], fr_v, 0)
    load(norm_gain, ng_v, 1)
    small = ((taps, taps_v), (cbias, vec_v.at[0]), (cgain, vec_v.at[1]), (cshift, vec_v.at[2]), (rate, hv_v.at[0]), (hgain, hv_v.at[1]))
    for n, (src, dst) in enumerate(small):
        load(src, dst, 2 + n)
    load(fw, w.at[:, pl.ds(FG, 128)], 8)
    load(iw, w.at[:, pl.ds(IN, 128)], 8)
    load(qw, w.at[:, pl.ds(QU, 128)], 9)
    load(gw, w.at[:, pl.ds(GA, 128)], 9)
    load(cvt, cwt.at[0, pl.ds(0, 64)], 10)
    load(cgt, cwt.at[1, pl.ds(0, 64)], 10)
    load(cow, wc.at[0, pl.ds(0, 64)], 11)
    load(row, wr.at[0, pl.ds(0, 128)], 12)
    wait_load(fr_v, 0)
    wait_load(ng_v, 1)

    values = fr_v[...].astype(F32)
    scale = lax.rsqrt(jnp.mean(values * values, axis=-1, keepdims=True) + EPS)
    xs[0] = (values * scale * ng_v[...]).astype(BF16)
    for n, (src, dst) in enumerate(small):
        wait_load(dst, 2 + n)
    pk[0] = jnp.zeros((40, 128), F32)
    pk[0, 0:TAPS, 0:64] = taps_v[...].astype(F32)
    for k in range(3):
        pk[0, 32 + k : 33 + k, 0:64] = vec_v[k]
    for k in range(2):
        pk[0, 35 + k : 36 + k, :] = hv_v[k]

    pl.semaphore_wait(
        bar,
        4 + ahead + pair + jnp.where((y == NY - 1) & (odd == 1) & (z < NZ - 1), 1, 0),
    )

    def half(ref, s, h):
        return ref.at[s, pl.ds(64 * h, 64)]

    g = [
        remote(half(xs, 0, 0), half(xs, 1, 0), gsend, grecv.at[0], at_x(1)),
        remote(half(xs, 0, 1), half(xs, 2, 1), gsend, grecv.at[1], at_x(-1)),
        remote(half(xs, 0, 1), half(xs, 1, 1), gsend, grecv.at[2], at_x(1)),
        remote(half(xs, 0, 0), half(xs, 2, 0), gsend, grecv.at[3], at_x(-1)),
        remote(half(xs, 1, 0), half(xs, 3, 0), gsend, grecv.at[4], at_x(1)),
        remote(half(xs, 2, 1), half(xs, 3, 1), gsend, grecv.at[5], at_x(-1)),
    ]
    for copy in g[:4]:
        copy.start()

    for dev, number in mates:

        @pl.when(rank(number) < rank(me))
        def _():
            signal(y_in, dev)

    @pl.loop(0, pair)
    def _(i):
        signal(z_in, {"z": 2 * i + odd})

    remote(fw, w.at[:, pl.ds(FG + 128, 128)], psend.at[0], precv.at[0], partner).start()
    remote(iw, w.at[:, pl.ds(IN + 128, 128)], psend.at[0], precv.at[0], partner).start()
    remote(pk.at[0], pk.at[1], psend.at[2], precv.at[3], partner).start()
    remote(cvt, cwt.at[0, pl.ds(64, 64)], psend.at[1], precv.at[2], partner).start()
    remote(cgt, cwt.at[1, pl.ds(64, 64)], psend.at[1], precv.at[2], partner).start()
    remote(qw, w.at[:, pl.ds(QU + 128, 128)], psend.at[0], precv.at[1], partner).start()
    remote(gw, w.at[:, pl.ds(GA + 128, 128)], psend.at[0], precv.at[1], partner).start()
    remote(cow, wc.at[0, pl.ds(64, 64)], psend.at[3], precv.at[4], partner).start()
    remote(row, wr.at[0, pl.ds(128, 128)], psend.at[4], precv.at[5], partner).start()

    wait_load(w.at[:, pl.ds(0, 256)], 8)
    wait_load(w.at[:, pl.ds(0, 256)], 9)
    wait_load(cwt.at[0], 10)
    arrived(w.at[:, pl.ds(0, 256)], precv.at[0])
    arrived(pk.at[1], precv.at[3])

    def conv_rows(a, b):
        return jnp.concatenate([pk[0, a:b, 0:64], pk[1, a:b, 0:64]], axis=1)

    tap_rows = conv_rows(0, 32)
    bias_row, gain_row, shift_row = (conv_rows(32 + k, 33 + k) for k in range(3))
    rate_row = jnp.concatenate([pk[0, 35:36], pk[1, 35:36]], axis=1) / SEQ_LEN
    hgain_row = jnp.concatenate([pk[0, 36:37], pk[1, 36:37]], axis=1)

    at_t = lax.broadcasted_iota(jnp.int32, (POS, POS), 0)
    at_u = lax.broadcasted_iota(jnp.int32, (POS, POS), 1)
    causal = at_u <= at_t
    tril = jnp.where(causal, 1.0, 0.0).astype(BF16)

    def spread(rows2):
        return jnp.concatenate(
            [jnp.broadcast_to(rows2[h : h + 1], (16, 128)) for h in range(2)], axis=0
        )

    def begin(j):
        rows = xs[j]
        forget_raw = dot(rows, w[:, FG : FG + 256]).astype(BF16).astype(F32)
        inputs = dot(rows, w[:, IN : IN + 256]).astype(BF16)
        in_gate = rate_row * sigmoid(-forget_raw)
        log_forget = jnp.log1p(-in_gate)
        hi = log_forget.astype(BF16)
        rest = log_forget - hi.astype(F32)
        mid = rest.astype(BF16)
        low = (rest - mid.astype(F32)).astype(BF16)
        cumulative = dot(tril, hi) + dot(tril, mid) + dot(tril, low)
        last = cumulative[POS - 1 : POS]
        weighted = (in_gate * jnp.exp(last - cumulative)).astype(BF16)
        for h in range(2):
            lanes = slice(128 * h, 128 * h + 128)
            state = lax.dot_general(
                inputs[:, lanes], weighted[:, lanes], TN, preferred_element_type=F32
            )
            for k in range(8):
                st_s[j, k, 16 * h : 16 * h + 16] = state[16 * k : 16 * k + 16]
            dec_s[j, h : h + 1] = jnp.exp(last[:, lanes])
        gt_b[j] = in_gate
        cum_b[j] = cumulative
        inp_b[j] = inputs

    def deal(j):
        for dev, to in mates:
            remote(st_s.at[j, to], st_r.at[j, me], r1s.at[0], r1r.at[j, 0], dev).start()
            remote(dec_s.at[j], dec_r.at[j, me], r1s.at[1], r1r.at[j, 1], dev).start()
        st_r[j, me] = st_s[j, me]
        dec_r[j, me] = dec_s[j]

    def gating(j):
        rows = xs[j]
        conv_value = lax.dot_general(rows, cwt[0], NT, preferred_element_type=F32)
        conv_gate = lax.dot_general(rows, cwt[1], NT, preferred_element_type=F32)
        conv_value = conv_value.astype(BF16).astype(F32)
        conv_gate = conv_gate.astype(BF16).astype(F32)
        gated = (conv_value * sigmoid(conv_gate)).astype(BF16)
        halo_s[j] = gated[POS - HALO :]
        ext[j, HALO:] = gated.astype(F32)

    def pass_on(j):
        @pl.when(y < NY - 1)
        def _():
            remote(halo_s.at[j], halo_r.at[j], hs, hr.at[j], {"y": y + 1}).start()

        @pl.when((y == NY - 1) & (z < NZ - 1))
        def _():
            remote(halo_s.at[j], halo_r.at[j], hs, hr.at[j], {"z": z + 1, "y": 0}).start()

    def within(j):
        rows = xs[j]
        queries = dot(rows, w[:, QU : QU + 256]).astype(BF16).astype(F32)
        cumulative = cum_b[j]
        grown = (queries * jnp.exp(cumulative)).astype(BF16)
        shrunk = (gt_b[j] * jnp.exp(-cumulative)).astype(BF16)
        grown_b[j] = grown
        for h in range(2):
            lanes = slice(128 * h, 128 * h + 128)
            scores = lax.dot_general(
                grown[:, lanes], shrunk[:, lanes], NT, preferred_element_type=F32
            )
            scores = jnp.where(causal, scores, 0.0).astype(BF16)
            local_b[j, :, lanes] = dot(scores, inp_b[j, :, lanes])
        gate_b[j] = dot(rows, w[:, GA : GA + 256]).astype(BF16)

    def totals(j):
        arrived(st_r.at[j, pl.ds(0, 7)], r1r.at[j, 0])
        arrived(dec_r.at[j, pl.ds(0, 7)], r1r.at[j, 1])
        total = st_r[j, 0]
        decay = dec_r[j, 0]
        for k in range(1, 8):
            total = total * spread(dec_r[j, k]) + st_r[j, k]
            decay = decay * dec_r[j, k]
        t_s[j] = total
        dd_s[j] = decay

        @pl.loop(pair + 1, 4)
        def _(i):
            dev = {"z": 2 * i + odd}
            remote(t_s.at[j], t_r.at[j, pair], r2s.at[0], r2r.at[j, 0], dev).start()
            remote(dd_s.at[j], dd_r.at[j, pair], r2s.at[1], r2r.at[j, 1], dev).start()

    def carry(j):
        for n in (1, 2, 3):

            @pl.when(pair == n)
            def _():
                arrived(t_r.at[j, pl.ds(0, n)], r2r.at[j, 0])
                arrived(dd_r.at[j, pl.ds(0, n)], r2r.at[j, 1])

        def step(i, state):
            return state * spread(dd_r[j, i]) + t_r[j, i]

        state = lax.fori_loop(0, pair, step, jnp.zeros((32, 128), F32))
        for k in range(8):
            c_s[j, k] = state.astype(BF16)
            if k < 7:
                state = state * spread(dec_r[j, k]) + st_r[j, k]
        for dev, to in mates:
            remote(c_s.at[j, to], c_r.at[j, me], r3s, r3r.at[j], dev).start()
        c_r[j, me] = c_s[j, me]

    def filtering(j):
        @pl.when((z > 0) | (y > 0))
        def _():
            arrived(halo_r.at[j], hr.at[j])
            ext[j, 0:HALO] = halo_r[j].astype(F32)

        @pl.when((z == 0) & (y == 0))
        def _():
            ext[j, 0:HALO] = jnp.zeros((HALO, 128), F32)

        acc = jnp.broadcast_to(bias_row, (POS, 128))
        for k in range(TAPS):
            first = HALO - (TAPS - 1) + k
            acc = acc + tap_rows[k : k + 1] * ext[j, first : first + POS]
        filt[j] = acc
        return jnp.sum(acc, axis=-1, keepdims=True), jnp.sum(acc * acc, axis=-1, keepdims=True)

    def conv_norm(j, sums, squares):
        mean = sums / D_CONV
        var = squares / D_CONV - mean * mean
        scaled = (filt[j] - mean) * lax.rsqrt(var + EPS) * gain_row + shift_row
        return (scaled * sigmoid(scaled)).astype(BF16)

    def finish(j):
        arrived(c_r.at[j, pl.ds(0, 7)], r3r.at[j])
        gate = gate_b[j].astype(F32)
        silu = gate * sigmoid(gate)
        parts = []
        for h in range(2):
            lanes = slice(128 * h, 128 * h + 128)
            low = jnp.concatenate([c_r[j, k, 16 * h : 16 * h + 16] for k in range(8)], axis=0)
            raw = local_b[j, :, lanes] + lax.dot_general(
                grown_b[j, :, lanes], low, NT, preferred_element_type=F32
            )
            scale = lax.rsqrt(jnp.mean(raw * raw, axis=-1, keepdims=True) + EPS)
            parts.append((raw * scale * hgain_row[:, lanes] * silu[:, lanes]).astype(BF16))
        return jnp.concatenate(parts, axis=1)

    def rec_half(s, h):
        return wr.at[s, pl.ds(64 * h, 64)]

    def conv_half(s, h):
        return wc.at[s, pl.ds(32 * h, 32)]

    def own(h):
        return row.at[pl.ds(64 * h, 64)], cow.at[pl.ds(32 * h, 32)]

    rs, cs = wxs.at[0], wxs.at[1]

    def send_own(k, h):
        s = SLOT_OF[-k % NX]
        a, b = own(h)
        remote(a, rec_half(s, h), rs, wxr.at[s, h, 0], at_x(k)).start()
        remote(b, conv_half(s, h), cs, wxr.at[s, h, 1], at_x(k)).start()

    def send_on(k, h):
        s = SLOT_OF[-k % NX]
        arrived(rec_half(s, h), wxr.at[s, h, 0])
        remote(rec_half(s, h), rec_half(3, h), rs, wxr.at[3, h, 0], at_x(k)).start()
        arrived(conv_half(s, h), wxr.at[s, h, 1])
        remote(conv_half(s, h), conv_half(3, h), cs, wxr.at[3, h, 1], at_x(k)).start()

    def over(s, halves):
        for h in halves:
            arrived(rec_half(s, h), wxr.at[s, h, 0])
            arrived(conv_half(s, h), wxr.at[s, h, 1])
        remote(wr.at[s, pl.ds(0, 128)], wr.at[s, pl.ds(128, 128)], wfs.at[0], wfr.at[0], partner).start()
        remote(wc.at[s, pl.ds(0, 64)], wc.at[s, pl.ds(64, 64)], wfs.at[1], wfr.at[1], partner).start()

    def spread_out(j, rows):
        if j == 0:
            ar_r[3] = rows
        else:
            ar_s[j - 1] = rows
            to = SLOT_OF[-OFF[j] % NX] - 1
            remote(ar_s.at[j - 1], ar_r.at[to], ars, arr.at[to], at_x(OFF[j])).start()

    begin(0)
    arrived(cwt.at[0], precv.at[2])
    gating(0)
    arrived(w.at[:, pl.ds(0, 256)], precv.at[1])
    within(0)
    behind = 7 - ahead

    @pl.when(behind > 0)
    def _():
        pl.semaphore_wait(y_in, behind)

    deal(0)
    pass_on(0)
    g[0].wait_recv()
    g[4].start()
    g[1].wait_recv()
    g[5].start()
    send_own(1, 0)
    send_own(-1, 1)
    send_own(1, 1)
    send_own(-1, 0)
    g[2].wait_recv()
    begin(1)
    deal(1)
    g[3].wait_recv()
    begin(2)
    deal(2)

    @pl.when(pair < 3)
    def _():
        pl.semaphore_wait(z_in, 3 - pair)

    totals(0)
    g[4].wait_recv()
    g[5].wait_recv()
    begin(3)
    deal(3)
    gating(1)
    pass_on(1)
    gating(2)
    pass_on(2)
    gating(3)
    pass_on(3)
    within(1)
    totals(1)
    totals(2)
    carry(0)
    within(2)
    within(3)
    sums = [filtering(j) for j in range(3)]
    totals(3)
    sums.append(filtering(3))
    lane = lax.broadcasted_iota(jnp.int32, (POS, 128), 1)
    packed = jnp.zeros((POS, 128), F32)
    for j in range(4):
        packed = jnp.where(lane == j, sums[j][0], packed)
        packed = jnp.where(lane == 4 + j, sums[j][1], packed)
    stat_s[...] = packed.T[0:8]
    for k in (1, -1, 2):
        remote(stat_s, stat_r.at[SLOT_OF[-k % NX] - 1], ss, sr, at_x(k)).start()
    send_on(1, 0)
    send_on(-1, 1)
    carry(1)
    carry(2)
    spread_out(0, finish(0))
    carry(3)
    arrived(stat_r, sr)
    total = stat_s[...]
    for s in (1, 2, 3):
        got = stat_r[s - 1]
        order = [SLOT_OF[(OFF[j] - OFF[s]) % NX] for j in range(4)]
        total = total + jnp.concatenate(
            [got[base + k : base + k + 1] for base in (0, 4) for k in order], axis=0
        )
    columns = jnp.concatenate([total, jnp.zeros((120, 128), F32)], axis=0).T
    for j in range(4):
        rows = conv_norm(j, columns[:, j : j + 1], columns[:, 4 + j : 5 + j])
        if j == 0:
            ac_r[3] = rows
        else:
            ac_s[j - 1] = rows
            remote(ac_s.at[j - 1], ac_r.at[SLOT_OF[-OFF[j] % NX] - 1], acs, acr, at_x(OFF[j])).start()
    over(1, (1,))
    over(2, (0,))
    for j in (1, 2):
        rows = finish(j)
        spread_out(j, rows)
    over(3, (0, 1))
    rows = finish(3)
    spread_out(3, rows)
    wait_load(wc.at[0, pl.ds(0, 64)], 11)
    wait_load(wr.at[0, pl.ds(0, 128)], 12)
    arrived(wc.at[0, pl.ds(0, 64)], precv.at[4])
    arrived(wr.at[0, pl.ds(0, 128)], precv.at[5])
    acc = dot(ac_r[3], wc[0]) + dot(ar_r[3], wr[0])
    arrived(wc.at[pl.ds(0, 3), pl.ds(0, 64)], wfr.at[1])
    arrived(ac_r.at[pl.ds(0, 3)], acr)
    for j in (1, 2, 3):
        acc = acc + dot(ac_r[j - 1], wc[j])
    arrived(wr.at[pl.ds(0, 3), pl.ds(0, 128)], wfr.at[0])
    for j in (1, 2, 3):
        arrived(ar_r.at[j - 1], arr.at[j - 1])
        acc = acc + dot(ar_r[j - 1], wr[j])
    out[0] = acc.astype(BF16)

    sent(w.at[:, pl.ds(0, 512)], psend.at[0])
    sent(cwt.at[0], psend.at[1])
    sent(pk.at[0], psend.at[2])
    sent(wc.at[0, pl.ds(0, 64)], psend.at[3])
    sent(wr.at[0, pl.ds(0, 128)], psend.at[4])
    sent(xs.at[pl.ds(0, 3)], gsend)
    sent(st_s.at[:, pl.ds(0, 7)], r1s.at[0])
    sent(dec_r.at[:, pl.ds(0, 7)], r1s.at[1])
    for n in (1, 2, 3):

        @pl.when(pair == 3 - n)
        def _():
            sent(t_r.at[pl.ds(0, n)], r2s.at[0])
            sent(dd_r.at[pl.ds(0, n)], r2s.at[1])

    sent(c_r.at[:, pl.ds(0, 7)], r3s)

    @pl.when((y < NY - 1) | (z < NZ - 1))
    def _():
        sent(halo_s, hs)

    sent(stat_r, ss)
    sent(ac_s, acs)
    sent(ar_s, ars)
    sent(wr.at[pl.ds(0, 3), pl.ds(0, 128)], wxs.at[0])
    sent(wc.at[pl.ds(0, 3), pl.ds(0, 64)], wxs.at[1])
    sent(wr.at[pl.ds(0, 3), pl.ds(0, 128)], wfs.at[0])
    sent(wc.at[pl.ds(0, 3), pl.ds(0, 64)], wfs.at[1])


def local(
    frames, norm_gain, conv_value_w, conv_gate_w, conv_taps, conv_bias, channel_gain, channel_shift,
    query_w, forget_w, input_w, gate_w, memory_rate, head_gain, conv_out_w, rec_out_w,
):
    dma = pltpu.SemaphoreType.DMA
    scratch = [
        pltpu.VMEM((POS, D), BF16),
        pltpu.VMEM((1, D), F32),
        pltpu.VMEM((TAPS, 64), BF16),
        pltpu.VMEM((3, 1, 64), F32),
        pltpu.VMEM((2, 1, 128), F32),
        pltpu.VMEM((2, 40, 128), F32),
        pltpu.VMEM((4, POS, D), BF16),
        pltpu.VMEM((D, 1024), BF16),
        pltpu.VMEM((2, 128, D), BF16),
        pltpu.VMEM((4, 128, D), BF16),
        pltpu.VMEM((4, 256, D), BF16),
        pltpu.VMEM((4, POS, 256), BF16),
        pltpu.VMEM((4, POS, 256), BF16),
        pltpu.VMEM((4, POS, 256), BF16),
        pltpu.VMEM((4, POS, 256), F32),
        pltpu.VMEM((4, POS, 256), F32),
        pltpu.VMEM((4, POS, 256), F32),
        pltpu.VMEM((4, 8, 32, 128), F32),
        pltpu.VMEM((4, 8, 32, 128), F32),
        pltpu.VMEM((4, 2, 128), F32),
        pltpu.VMEM((4, 8, 2, 128), F32),
        pltpu.VMEM((4, 32, 128), F32),
        pltpu.VMEM((4, 4, 32, 128), F32),
        pltpu.VMEM((4, 2, 128), F32),
        pltpu.VMEM((4, 4, 2, 128), F32),
        pltpu.VMEM((4, 8, 32, 128), BF16),
        pltpu.VMEM((4, 8, 32, 128), BF16),
        pltpu.VMEM((4, HALO, 128), BF16),
        pltpu.VMEM((4, HALO, 128), BF16),
        pltpu.VMEM((4, HALO + POS, 128), F32),
        pltpu.VMEM((4, POS, 128), F32),
        pltpu.VMEM((8, 128), F32),
        pltpu.VMEM((3, 8, 128), F32),
        pltpu.VMEM((3, POS, 128), BF16),
        pltpu.VMEM((4, POS, 128), BF16),
        pltpu.VMEM((3, POS, 256), BF16),
        pltpu.VMEM((4, POS, 256), BF16),
        dma((13,)),
        dma((5,)), dma((6,)),
        dma(()), dma((6,)),
        dma((2,)), dma((4, 2)),
        dma((2,)), dma((4, 2)),
        dma(()), dma((4,)),
        dma(()), dma((4,)),
        dma(()), dma(()),
        dma(()), dma(()),
        dma(()), dma((3,)),
        dma((2,)), dma((4, 2, 2)),
        dma((2,)), dma((2,)),
        pltpu.SemaphoreType.REGULAR, pltpu.SemaphoreType.REGULAR,
    ]
    anywhere = pl.BlockSpec(memory_space=pltpu.HBM)
    return pl.pallas_call(
        kernel,
        out_shape=jax.ShapeDtypeStruct((1, POS, D), BF16),
        in_specs=[anywhere] * 16,
        out_specs=pl.BlockSpec(memory_space=pltpu.VMEM),
        scratch_shapes=scratch,
        compiler_params=pltpu.CompilerParams(
            collective_id=0, has_side_effects=True, vmem_limit_bytes=24 * 1024 * 1024
        ),
        name="mixer",
    )(*[pltpu.with_memory_space_constraint(a, pltpu.HBM) for a in (
        frames, norm_gain.reshape(1, -1), conv_value_w.T, conv_gate_w.T, conv_taps,
        conv_bias.reshape(1, -1), channel_gain.reshape(1, -1), channel_shift.reshape(1, -1),
        query_w, forget_w, input_w, gate_w, memory_rate.reshape(1, -1), head_gain.reshape(1, -1),
        conv_out_w, rec_out_w,
    )])


def solution(mesh):
    torus = Mesh(mesh.devices.reshape(NZ, NY, NX, 2), ("z", "y", "x", "c"))
    tp, sp = ("x", "c"), ("z", "y")
    columns, rows, vector = P(None, tp), P(tp, None), P(tp)
    in_specs = (
        P(tp, sp, None), P(), columns, columns, columns, vector, vector, vector,
        columns, columns, columns, columns, vector, vector, rows, rows,
    )
    return jax.shard_map(
        local, mesh=torus, in_specs=in_specs, out_specs=P(tp, sp, None), check_vma=False
    )
```
